256 devices in a mesh: st: 32 (over z, x), tp: 8 (over y, core).
Axes of the slice: x: 4, y: 4, z: 8, core: 2. Of those that a mesh axis runs over, the one named last changes fastest.
Arguments:
- tokens: bfloat16 [16384, 2048], P('st'), may hold values from -6 to 6
- mix_query: bfloat16 [2048, 1024], P(None, 'tp'), may hold values from -0.125 to 0.125
- mix_key: bfloat16 [2048, 1024], P(None, 'tp'), may hold values from -0.125 to 0.125
- mix_value: bfloat16 [2048, 1024], P(None, 'tp'), may hold values from -0.125 to 0.125
- decay_lower_map: bfloat16 [2048, 64], replicated, may hold values from -0.125 to 0.125
- decay_upper_map: bfloat16 [64, 1024], P(None, 'tp'), may hold values from -1 to 1
- decay_base: float32 [1024], P('tp'), may hold values from -7.5 to -2.5
- decay_shift: float32 [16384, 16], P('st', 'tp'), may hold values from -3.8 to 9.8
- rate_lower_map: bfloat16 [2048, 64], replicated, may hold values from -0.125 to 0.125
- rate_upper_map: bfloat16 [64, 1024], P(None, 'tp'), may hold values from -0.75 to 0.75
- norm_gain: float32 [1024], P('tp'), may hold values from 0.1 to 1.9
- mix_out: bfloat16 [1024, 2048], P(None, 'tp'), may hold values from -0.1875 to 0.1875
- cross_query: bfloat16 [2048, 2048], P(None, 'tp'), may hold values from -0.125 to 0.125
- score_gain: float32 [2048], P('tp'), may hold values from 0.1 to 1.9
- passage_key: bfloat16 [2048, 2048], P(None, 'tp'), may hold values from -0.125 to 0.125
- passage_value: bfloat16 [2048, 2048], P(None, 'tp'), may hold values from -0.125 to 0.125
- cross_out: bfloat16 [2048, 2048], P(None, 'tp'), may hold values from -0.5 to 0.5
- gate_down: bfloat16 [2048, 128], replicated, may hold values from -0.125 to 0.125
- gate_up: bfloat16 [128, 2048], P(None, 'tp'), may hold values from -0.5 to 0.5
- store: bfloat16 [384, 96, 2048], P('st'), may hold values from -6 to 6
- passage_ids: int32 [256, 4], P('st'), may hold values from 0 to 383, as said below
Outputs:
- mixed: bfloat16 [16384, 2048], P('st', 'tp')
The draws below stay inside these ranges and needn't reach their ends.
Inputs may be any that keep to these rules, and one draw needn't show every extreme that they name: `passage_ids`: among the 32 passages named by the rows of one sequence, at most 2 are held by one index of st (passage p by index p // 12); in every draw exactly 2 are held by the index before the sequence's own.
All inputs are finite; a program needn't handle non-finite values.
Results may differ from the reference program's by a relative error of at most 0.0075.
Values may be sent and summed in bfloat16 or wider, within the bound.
A program may use at most 128 MiB of HBM per device.

```python
import jax
import jax.numpy as jnp
from jax import lax

MODEL_DIM = 2048
MIXER_HEADS = 16
RHEAD = 64
XHEADS = 8
XHEAD = 256
LOWRANK_WIDTH = 64
GLORA = 128
PLEN = 96
PER_BLOCK = 4
QBLOCK = 64
MBLOCK = 64
TOKENS_PER_SEQ = 512
PASS_DEV = 12
MIXER_WIDTH = 1024
XWIDTH = 2048
TOKEN_TOTAL = 16384
NPASS = 384
N_ST = 32


def draw_decay_shift(key, part):
    sequence_number = TOKEN_TOTAL // TOKENS_PER_SEQ
    span_count = TOKENS_PER_SEQ // MBLOCK
    base_key, spot_key, random_size_key = jax.random.split(key, 3)
    shift_baseline = jax.random.uniform(base_key, (sequence_number, span_count, 1, 1), jnp.float32, -0.8, 0.8)
    shift_baseline = jnp.broadcast_to(shift_baseline, (sequence_number, span_count, MBLOCK, MIXER_HEADS))
    shift_baseline = shift_baseline.reshape(sequence_number, TOKENS_PER_SEQ, MIXER_HEADS)
    spot_pos = jax.random.randint(spot_key, (sequence_number, 3, MIXER_HEADS), 0, TOKENS_PER_SEQ)
    target_location = jnp.arange(TOKENS_PER_SEQ)[None, :, None, None] == spot_pos[:, None, :, :]
    spike_addition = jnp.any(target_location, axis=2).astype(jnp.float32)
    spike_addition = spike_addition * jax.random.uniform(random_size_key, (sequence_number, TOKENS_PER_SEQ, MIXER_HEADS), jnp.float32, 7.0, 9.0)
    return (shift_baseline + spike_addition).reshape(TOKEN_TOTAL, MIXER_HEADS)


def draw_passage_ids(key, part):
    blk_dev = TOKENS_PER_SEQ // QBLOCK
    slot_count = blk_dev * PER_BLOCK
    capacity = max(2, -(-slot_count // N_ST))
    positions = N_ST * capacity

    def one_sequence(seq_key, seq_index):
        keys_five = jax.random.split(seq_key, 5)
        place = jnp.arange(positions)
        offset = place // capacity
        copy_idx = place % capacity
        forced = (offset == N_ST - 1) | (offset == N_ST // 2) & (copy_idx == 0)
        score = jax.random.randint(keys_five[0], (positions,), 0, 1 << 20)
        score = jnp.where(forced, -1, score) * positions + place
        chosen = jnp.argsort(score)[:slot_count]
        owner_of = (seq_index + offset[chosen]) % N_ST
        mixing = jax.random.randint(keys_five[1], (slot_count,), 0, 1 << 20) * slot_count + jnp.arange(slot_count)
        owner_of = owner_of[jnp.argsort(mixing)]
        local_idx = jax.random.randint(keys_five[2], (slot_count,), 0, PASS_DEV)
        local_idx = jnp.minimum(local_idx, jax.random.randint(keys_five[3], (slot_count,), 0, PASS_DEV))
        local_idx = jnp.minimum(local_idx, jax.random.randint(keys_five[4], (slot_count,), 0, PASS_DEV))
        return (owner_of * PASS_DEV + local_idx).reshape(blk_dev, PER_BLOCK)
    seq_keys = jax.random.split(jax.random.fold_in(key, 11), N_ST)
    picked = jax.vmap(one_sequence)(seq_keys, jnp.arange(N_ST))
    return picked.reshape(N_ST * blk_dev, PER_BLOCK).astype(jnp.int32)


def block_levels(own_key, shape, shards, least, high):
    factor_of = 1.0
    for dim, blocks in shards:
        heights = jax.random.uniform(jax.random.fold_in(jax.random.fold_in(own_key, 6), dim), (blocks,), jnp.float32, least / len(shards), high / len(shards))
        factor_of = factor_of * jnp.repeat(jnp.exp(heights), shape[dim] // blocks).reshape((-1,) + (1,) * (len(shape) - 1 - dim))
    return factor_of


def noise(own_key, shape, width, bound, cuts=(), dtype=jnp.bfloat16):
    level = block_levels(own_key, shape, cuts, -0.22, 0.18) if cuts else 1.0
    entries = jax.random.normal(own_key, shape, jnp.float32) * width * level
    return jnp.minimum(jnp.maximum(entries, -bound), bound).astype(dtype)


def setup_inputs(seed: int = 0) -> dict:
    keys = jax.random.split(jax.random.key(seed), 22)
    tokens = noise(keys[0], (TOKEN_TOTAL, MODEL_DIM), 1.0, 6.0, ((0, 32),))
    mix_query = noise(keys[1], (MODEL_DIM, MIXER_WIDTH), MODEL_DIM ** -0.5, 0.125, ((1, 8),))
    mix_key = noise(keys[2], (MODEL_DIM, MIXER_WIDTH), MODEL_DIM ** -0.5, 0.125, ((1, 8),))
    mix_value = noise(keys[3], (MODEL_DIM, MIXER_WIDTH), MODEL_DIM ** -0.5, 0.125, ((1, 8),))
    decay_lower_map = noise(keys[4], (MODEL_DIM, LOWRANK_WIDTH), MODEL_DIM ** -0.5, 0.125)
    decay_upper_map = noise(keys[5], (LOWRANK_WIDTH, MIXER_WIDTH), (LOWRANK_WIDTH // 2) ** -0.5, 1.0, ((1, 8),))
    decay_base = jnp.clip(-7.5 + 5.0 * jax.random.uniform(keys[6], (MIXER_WIDTH,), jnp.float32) ** block_levels(keys[6], (MIXER_WIDTH,), ((0, 8),), -0.2, 0.2), -7.5, -2.5)
    decay_shift = draw_decay_shift(jax.random.fold_in(keys[21], 71), 0)
    rate_lower_map = noise(keys[8], (MODEL_DIM, LOWRANK_WIDTH), MODEL_DIM ** -0.5, 0.125)
    rate_upper_map = noise(keys[9], (LOWRANK_WIDTH, MIXER_WIDTH), LOWRANK_WIDTH ** -0.5, 0.75, ((1, 8),))
    norm_gain = jnp.clip(1.0 + 0.18 * jax.random.normal(keys[10], (MIXER_WIDTH,), jnp.float32), 0.1, 1.9)
    mix_out = noise(keys[11], (MIXER_WIDTH, MODEL_DIM), MIXER_WIDTH ** -0.5, 0.1875, ((1, 8),))
    cross_query = noise(keys[12], (MODEL_DIM, XWIDTH), MODEL_DIM ** -0.5, 0.125, ((1, 8),))
    score_gain = jnp.clip(1.0 + 0.18 * jax.random.normal(keys[13], (XWIDTH,), jnp.float32), 0.1, 1.9)
    passage_key = noise(keys[14], (MODEL_DIM, XWIDTH), MODEL_DIM ** -0.5, 0.125, ((1, 8),))
    passage_value = noise(keys[15], (MODEL_DIM, XWIDTH), MODEL_DIM ** -0.5, 0.125, ((1, 8),))
    cross_out = noise(keys[16], (XWIDTH, MODEL_DIM), (XWIDTH // 16) ** -0.5, 0.5, ((1, 8),))
    gate_down = noise(keys[17], (MODEL_DIM, GLORA), MODEL_DIM ** -0.5, 0.125)
    gate_up = noise(keys[18], (GLORA, MODEL_DIM), GLORA ** -0.5, 0.5, ((1, 8),))
    store = noise(keys[19], (NPASS, PLEN, MODEL_DIM), 1.0, 6.0, ((0, 32),))
    passage_ids = draw_passage_ids(jax.random.fold_in(keys[21], 71), 0)
    return dict(tokens=tokens, mix_query=mix_query, mix_key=mix_key, mix_value=mix_value, decay_lower_map=decay_lower_map, decay_upper_map=decay_upper_map, decay_base=decay_base, decay_shift=decay_shift, rate_lower_map=rate_lower_map, rate_upper_map=rate_upper_map, norm_gain=norm_gain, mix_out=mix_out, cross_query=cross_query, score_gain=score_gain, passage_key=passage_key, passage_value=passage_value, cross_out=cross_out, gate_down=gate_down, gate_up=gate_up, store=store, passage_ids=passage_ids)


FLOAT32 = jnp.float32
BFLOAT = jnp.bfloat16
PRECISE = lax.Precision.HIGHEST

def rounded(values):
    return lax.optimization_barrier(values.astype(BFLOAT)).astype(FLOAT32)

def head_norm(values, head_size):
    shaped = values.reshape(values.shape[:-1] + (values.shape[-1] // head_size, head_size))
    scaled = shaped * lax.rsqrt(lax.optimization_barrier(jnp.mean(shaped * shaped, axis=-1, keepdims=True)) + 1e-06)
    return scaled.reshape(values.shape)

def recurrent_step(state, inputs):
    query_vec, fade_t, key_vec, value_vec, unit_key, rate_gate = inputs
    pulled = jnp.einsum('bhij,bhj->bhi', state, -unit_key, precision=PRECISE)
    state = state * fade_t[:, :, None, :] + pulled[..., :, None] * (unit_key * rate_gate)[..., None, :] + value_vec[..., :, None] * key_vec[..., None, :]
    return (state, jnp.einsum('bhij,bhj->bhi', state, query_vec, precision=PRECISE))

def reference(tokens, mix_query, mix_key, mix_value, decay_lower_map, decay_upper_map, decay_base, decay_shift, rate_lower_map, rate_upper_map, norm_gain, mix_out, cross_query, score_gain, passage_key, passage_value, cross_out, gate_down, gate_up, store, passage_ids):
    total_rows = tokens.shape[0]
    sequence_number = total_rows // TOKENS_PER_SEQ

    def project(weight):
        return rounded(jnp.dot(tokens, weight, preferred_element_type=FLOAT32))
    query_vec = project(mix_query)
    key_vec = project(mix_key)
    value_vec = project(mix_value)
    decay_low = jnp.tanh(jnp.dot(tokens, decay_lower_map, preferred_element_type=FLOAT32)).astype(BFLOAT)
    decay_pre = decay_base + jnp.dot(decay_low, decay_upper_map, preferred_element_type=FLOAT32) + jnp.repeat(decay_shift, RHEAD, axis=1)
    log_fade = -jnp.exp(-jax.nn.softplus(-decay_pre) - 0.5)
    rate_low = jnp.dot(tokens, rate_lower_map, preferred_element_type=FLOAT32).astype(BFLOAT)
    rate_gate = jax.nn.sigmoid(jnp.dot(rate_low, rate_upper_map, preferred_element_type=FLOAT32))

    def by_time(values):
        return jnp.moveaxis(values.reshape(sequence_number, TOKENS_PER_SEQ, MIXER_HEADS, RHEAD), 1, 0)
    keyed = key_vec.reshape(total_rows, MIXER_HEADS, RHEAD)
    unit_key = keyed * lax.rsqrt(lax.optimization_barrier(jnp.sum(keyed * keyed, axis=-1, keepdims=True)) + 1e-06)
    sequence_in = (by_time(query_vec), by_time(jnp.exp(log_fade)), by_time(key_vec), by_time(value_vec), by_time(unit_key), by_time(rate_gate))
    state_zero = jnp.zeros((sequence_number, MIXER_HEADS, RHEAD, RHEAD), FLOAT32)
    _, head_out = lax.scan(recurrent_step, state_zero, sequence_in)
    head_out = jnp.moveaxis(head_out, 0, 1).reshape(total_rows, MIXER_HEADS, RHEAD)
    centred = head_out - lax.optimization_barrier(jnp.mean(head_out, axis=-1, keepdims=True))
    spread = lax.optimization_barrier(jnp.mean(centred * centred, axis=-1, keepdims=True))
    mixer_heads = (centred * lax.rsqrt(spread + 0.00064)).reshape(total_rows, MIXER_WIDTH)
    mixer_heads = (mixer_heads * norm_gain).astype(BFLOAT)
    queries = head_norm(jnp.dot(tokens, cross_query, preferred_element_type=FLOAT32), XHEAD) * score_gain
    queries = queries.astype(BFLOAT)
    store_rows = store.reshape(-1, MODEL_DIM)
    keys_all = head_norm(jnp.dot(store_rows, passage_key, preferred_element_type=FLOAT32), XHEAD)
    keys_all = keys_all.astype(BFLOAT).reshape(-1, PLEN, XWIDTH)
    values_all = jnp.dot(store_rows, passage_value, preferred_element_type=FLOAT32).astype(BFLOAT)
    values_all = values_all.reshape(-1, PLEN, XWIDTH)

    def attend(item):
        block_q, block_ids = item
        block_keys = keys_all[block_ids].reshape(-1, XHEADS, XHEAD).astype(FLOAT32)
        block_values = values_all[block_ids].reshape(-1, XHEADS, XHEAD).astype(FLOAT32)
        block_q = block_q.reshape(QBLOCK, XHEADS, XHEAD).astype(FLOAT32)
        scores = jnp.einsum('qhd,khd->hqk', block_q, block_keys, precision=PRECISE) * XHEAD ** (-0.5)
        expon = jnp.exp(scores)
        weights = rounded(expon / lax.optimization_barrier(jnp.sum(expon, axis=-1, keepdims=True)))
        result = jnp.einsum('hqk,khd->qhd', weights, block_values, precision=PRECISE)
        return result.astype(BFLOAT).reshape(QBLOCK, XWIDTH)
    attended = lax.map(attend, (queries.reshape(-1, QBLOCK, XWIDTH), passage_ids)).reshape(total_rows, XWIDTH)
    gate_low = jnp.dot(tokens, gate_down, preferred_element_type=FLOAT32).astype(BFLOAT)
    gate_open = jax.nn.sigmoid(jnp.dot(gate_low, gate_up, preferred_element_type=FLOAT32))
    mixer_part = jnp.dot(mixer_heads, mix_out, preferred_element_type=FLOAT32)
    cross_part = jnp.dot(attended, cross_out, preferred_element_type=FLOAT32)
    return (mixer_part + gate_open * cross_part).astype(BFLOAT)
```

```python
import functools
import math

import jax
import jax.numpy as jnp
from jax import lax
from jax.experimental import pallas as pl
from jax.experimental.pallas import tpu as pltpu
from jax.sharding import PartitionSpec as P

F32 = jnp.float32
BF = jnp.bfloat16
NZ, NX = 8, 4
QBLOCK = 64
VMEM = pl.BlockSpec(memory_space=pltpu.VMEM)
MESH = pl.DeviceIdType.MESH
HBM = pl.BlockSpec(memory_space=pltpu.HBM)
SMEM = pl.BlockSpec(memory_space=pltpu.SMEM)
ANY = pl.BlockSpec(memory_space=pl.ANY)


def dg(a, b, ca, cb):
    return lax.dot_general(a, b, (((ca,), (cb,)), ((), ())), preferred_element_type=F32)


def bdot(a, b, ca=1, cb=0):
    return dg(a.astype(BF), b.astype(BF), ca, cb)


def cost(flops):
    return pl.CostEstimate(flops=int(flops), bytes_accessed=int(4e6), transcendentals=0)


def params(mib, **kw):
    return pltpu.CompilerParams(vmem_limit_bytes=mib * 1024 * 1024, **kw)


def head_normed(y):
    return y * lax.rsqrt(jnp.mean(y * y, axis=-1, keepdims=True) + 1e-06)


def exact_sum_dot(left, x, ca, cb, swap):
    hi = x.astype(BF)
    r = x - hi.astype(F32)
    mid = r.astype(BF)
    low = (r - mid.astype(F32)).astype(BF)
    parts = [dg(p, left, ca, cb) if swap else dg(left, p, ca, cb) for p in (hi, mid, low)]
    return parts[0] + parts[1] + parts[2]


def mixer_stages(tok, wq, wk, wv, wdl, wdu, base, shift, wrl, wru, gain, out,
                 s_a, s_q, s_ki, s_ri, s_kf, s_rf, s_vs, s_e, s_o):
    t = tok[...]
    rows = t.shape[0]
    chunks = rows // 64
    lane = lax.broadcasted_iota(jnp.int32, (64, 128), 1)
    row = lax.broadcasted_iota(jnp.int32, (64, 128), 0)
    left = lane < 64
    in_head = jnp.where(left, lane, lane - 64)
    sl = left & (in_head < row)
    sr = jnp.logical_not(left) & (in_head < row)
    upto = in_head <= row
    r2 = lax.broadcasted_iota(jnp.int32, (128, 128), 0)
    l2 = lax.broadcasted_iota(jnp.int32, (128, 128), 1)
    same = (r2 < 64) == (l2 < 64)
    eye = r2 == l2
    ones = jnp.where(same, 1.0, 0.0).astype(BF)
    tri = jnp.where(
        lax.broadcasted_iota(jnp.int32, (64, 64), 1) <= lax.broadcasted_iota(jnp.int32, (64, 64), 0),
        1.0, 0.0).astype(BF)
    q = dg(t, wq[...], 1, 0).astype(BF).astype(F32)
    k = dg(t, wk[...], 1, 0).astype(BF).astype(F32)
    v = dg(t, wv[...], 1, 0).astype(BF).astype(F32)
    low = jnp.tanh(dg(t, wdl[...], 1, 1)).astype(BF)
    spread2 = jnp.where(
        (lax.broadcasted_iota(jnp.int32, (2, 128), 1) < 64)
        == (lax.broadcasted_iota(jnp.int32, (2, 128), 0) == 0), 1.0, 0.0).astype(BF)
    pre = base[...] + dg(low, wdu[...], 1, 0) + exact_sum_dot(spread2, shift[...], 0, 0, True)
    log_fade = jax.nn.sigmoid(pre) * (-math.exp(-0.5))
    rate_low = dg(t, wrl[...], 1, 1).astype(BF)
    rate = jax.nn.sigmoid(dg(rate_low, wru[...], 1, 0))
    unit = k * lax.rsqrt(exact_sum_dot(ones, k * k, 1, 0, True) + 1e-06)
    rate_key = unit * rate
    s_vs[...] = pltpu.roll(v, 64, 1).astype(BF)
    for c in range(chunks):
        s = slice(64 * c, 64 * c + 64)
        f = log_fade[s]
        cumul = exact_sum_dot(tri, f, 1, 0, False)
        end = cumul[63:64]
        ei = jnp.exp(-cumul)
        fo = jnp.exp(end - cumul)
        s_a[s, :] = -unit[s] * jnp.exp(cumul - f)
        s_q[s, :] = q[s] * jnp.exp(cumul)
        s_ki[s, :] = (k[s] * ei).astype(BF)
        s_ri[s, :] = (rate_key[s] * ei).astype(BF)
        s_kf[s, :] = (k[s] * fo).astype(BF)
        s_rf[s, :] = (rate_key[s] * fo).astype(BF)
        s_e[c:c + 1, :] = jnp.exp(end)

    yield
    zb = jnp.zeros((64, 128), BF)
    zf = jnp.zeros((64, 128), F32)

    def only(x, m):
        return jnp.where(m, x, zb if x.dtype == BF else zf)

    right = jnp.logical_not(left)
    cat = jnp.concatenate
    group = 4
    state = jnp.zeros((128, 128), F32)
    for g in range(chunks // group):
        cs = [slice(64 * c, 64 * c + 64) for c in range(g * group, (g + 1) * group)]
        G0, G1, PW, X, VL, VR = [], [], [], [], [], []
        for s in cs:
            a, qq = s_a[s, :].astype(BF), s_q[s, :].astype(BF)
            ki, ri = s_ki[s, :], s_ri[s, :]
            G0.append(dg(cat([only(a, left), only(qq, left)], 0), cat([ri, ki], 0), 1, 1))
            G1.append(dg(cat([only(a, right), only(qq, right)], 0), cat([ki, ri], 0), 1, 1))
        for i, s in enumerate(cs):
            vs = s_vs[s, :]
            VR.append(only(vs, right))
            VL.append(only(vs, left))
            L = cat([only(G0[i][:64], sr), only(G1[i][:64], sl)], 0)
            PW.append(cat([only(G0[i][:64], sl), only(G1[i][:64], sr)], 0))
            a = s_a[s, :]
            X.append(cat([only(a, left), only(a, right)], 0) + bdot(L, cat([VL[i], VR[i]], 0)))
        for it in range(6):
            for i in range(group):
                p16 = PW[i].astype(BF)
                if it < 5:
                    px = dg(p16, cat([p16, X[i].astype(BF)], 1), 1, 0)
                    PW[i] = px[:, :128]
                    X[i] = X[i] + px[:, 128:]
                else:
                    X[i] = X[i] + dg(p16, X[i].astype(BF), 1, 0)
        MM, NN, PC, OO = [], [], [], []
        for i, s in enumerate(cs):
            x16 = X[i].astype(BF)
            h0 = cat([x16[:64], VR[i]], 0)
            h1 = cat([VL[i], x16[64:]], 0)
            y0 = bdot(only(G0[i][64:], upto), h0)
            y1 = bdot(only(G1[i][64:], upto), h1)
            qq = s_q[s, :]
            PC.append(cat([only(y0 + qq, left), only(y1 + qq, right)], 0).astype(BF))
            OO.append(only(y0, right) + only(y1, left))
            kf, rf = s_kf[s, :], s_rf[s, :]
            f = cat([only(rf, left), only(kf, left), only(kf, right), only(rf, right)], 0)
            tr = dg(cat([h0, h1], 0), f, 0, 0)
            e = s_e[g * group + i:g * group + i + 1, :]
            zz = jnp.zeros((128, 128), F32)
            MM.append((jnp.where(same, tr, zz) + jnp.where(eye, e, zz)).astype(BF))
            NN.append(jnp.where(same, zz, tr))
        for i, s in enumerate(cs):
            s16 = state.astype(BF)
            o = dg(PC[i], s16, 1, 1)
            s_o[s, :] = OO[i] + o[:64] + o[64:]
            state = dg(s16, MM[i], 1, 0) + NN[i]
        yield
    o = pltpu.roll(s_o[...], 64, 1)
    centred = o - exact_sum_dot(ones, o, 1, 0, True) * (1.0 / 64)
    spread = exact_sum_dot(ones, centred * centred, 1, 0, True) * (1.0 / 64)
    out[...] = (centred * lax.rsqrt(spread + 0.00064) * gain[...]).astype(BF)


ORDER = (0, 1, 6, 7, 2, 3, 8, 9, 4, 5, 10, 11)


def remote(src, dst, send, recv, **device):
    return pltpu.make_async_remote_copy(
        src_ref=src, dst_ref=dst, send_sem=send, recv_sem=recv, device_id=device,
        device_id_type=MESH)


def meet(peers):
    barrier = pltpu.get_barrier_semaphore()
    for device in peers:
        pl.semaphore_signal(barrier, inc=1, device_id=device, device_id_type=MESH)
    return lambda: pl.semaphore_wait(barrier, len(peers))


def slot_list(ids, z, x):
    row = lax.broadcasted_iota(jnp.int32, (64, 128), 0)
    lane = lax.broadcasted_iota(jnp.int32, (64, 128), 1)
    valid = (row - 8 * (row // 8) < 4) & (lane < 8)
    p = ids.reshape(64, 128).astype(F32)
    plane = jnp.floor((p + 0.5) * (1.0 / 48))
    owner = jnp.floor((p + 0.5) * (1.0 / 12))
    step = owner - 4 * plane - x.astype(F32)
    step = jnp.where(step < 0, step + 4, step)
    slot = step * 12 + p - 12 * owner
    hit = valid & (plane == z.astype(F32))
    m = jnp.where(hit, 1.0, 0.0)
    r1 = lax.broadcasted_iota(jnp.int32, (64, 64), 0)
    c1 = lax.broadcasted_iota(jnp.int32, (64, 64), 1)
    r2 = lax.broadcasted_iota(jnp.int32, (128, 128), 0)
    c2 = lax.broadcasted_iota(jnp.int32, (128, 128), 1)
    near = r1 // 8 == c1 // 8
    above = bdot(jnp.where(near & (c1 < r1), 1.0, 0.0), m)
    column = bdot(jnp.where(near, 1.0, 0.0), m)
    pos = above + bdot(column, jnp.where(r2 < c2, 1.0, 0.0))
    pos = jnp.where(hit, pos, -1.0)
    lanes = lane.astype(F32)
    acc = jnp.zeros((64, 128), F32)
    for b in range(8):
        at = pos[:, b:b + 1]
        acc = acc + jnp.where(at == lanes, slot[:, b:b + 1], 0.0)
        acc = acc + jnp.where((at == lanes - 64) & (at >= 0), b + 1.0, 0.0)
    return jnp.sum(acc.reshape(8, 8, 128), axis=1).astype(jnp.int32)


PIPES = (("st_up", 0, (4, 3, 2, 1)), ("st_down", 1, (4, 5, 6, 7)),
         ("st_up", 1, (3, 2, 1)), ("st_down", 0, (5, 6, 7)))


class Spread:
    def __init__(self, own, buf, send, recv, yp, ym, sib):
        self.copies = []
        for h in range(2):
            s = own.at[pl.ds(256 * h, 256), :]
            links = [(s, buf.at[1, 0, h], sib), (s, buf.at[0, 3, h], yp), (s, buf.at[0, 1, h], ym),
                     (buf.at[0, 3, h], buf.at[1, 3, h], sib), (buf.at[0, 1, h], buf.at[1, 1, h], sib),
                     (buf.at[0, 3, h], buf.at[0, 2, h], yp) if h == 0
                     else (buf.at[0, 1, h], buf.at[0, 2, h], ym),
                     (buf.at[0, 2, h], buf.at[1, 2, h], sib)]
            self.copies.append([
                remote(a, b, send.at[h, k], recv.at[h, k], tp=to) for k, (a, b, to) in enumerate(links)])

    def first(self, h):
        c = self.copies[h]
        for k in ((1, 2, 0) if h == 0 else (2, 1, 0)):
            c[k].start()

    def second(self, h):
        c = self.copies[h]
        if h == 0:
            c[1].wait_recv()
            c[5].start()
            c[3].start()
            c[2].wait_recv()
            c[4].start()
        else:
            c[2].wait_recv()
            c[5].start()
            c[4].start()
            c[1].wait_recv()
            c[3].start()

    def third(self, h):
        self.copies[h][5].wait_recv()
        self.copies[h][6].start()

    def arrived(self, h, *which):
        for k in which:
            self.copies[h][k].wait_recv()

    def finish(self):
        for c in self.copies[0] + self.copies[1]:
            c.wait_send()


def layer_kernel(store, wk, wv, tok, wq, wg, mq, mk, mv, wc, wm, wgu, qgain, ids, wdl, wdu, base, shift, wrl,
                 wru, gain, out,
                 sv, wkv, wvv, tokv, wqv, wgv, mqv, mkv, mvv, wcv, wmv, wguv, kvs, qq, idv, lstv, lst,
                 glow, heads, s_a, s_q, s_ki, s_ri, s_kf, s_rf, s_vs, s_e, s_o,
                 kd, vd, part, den, msg, box, head_all, att, att_all, gate, mixed,
                 in_sem, xs, xr, zs, zr, ids_s, ids_r, ps, pr, hs, hr, as_, ar):
    st, tp = lax.axis_index("st"), lax.axis_index("tp")
    z, x = st // NX, lax.rem(st, NX)
    y, core = tp // 2, lax.rem(tp, 2)
    xp = z * NX + lax.rem(x + 1, NX)
    xm = z * NX + lax.rem(x + NX - 1, NX)
    zp = lax.rem(z + 1, NZ) * NX + x
    zm = lax.rem(z + NZ - 1, NZ) * NX + x
    yp = lax.rem(y + 1, 4) * 2 + core
    ym = lax.rem(y + 3, 4) * 2 + core
    sib = y * 2 + 1 - core
    ready = meet([{"st": xp}, {"st": xm}, {"st": zp}, {"st": zm}, {"tp": yp}, {"tp": ym}, {"tp": sib}])
    loads = {}

    def load(name, src, dst):
        loads[name] = pltpu.make_async_copy(src, dst, in_sem.at[len(loads)])
        loads[name].start()

    load("wk", wk, wkv)
    load("wv", wv, wvv)
    for p, i in enumerate(ORDER):
        load(i, store.at[i], sv.at[p])
    for name, src, dst in (("tok", tok, tokv), ("wq", wq, wqv), ("wg", wg, wgv), ("mq", mq, mqv),
                           ("mk", mk, mkv), ("mv", mv, mvv), ("wm", wm, wmv), ("wgu", wgu, wguv),
                           ("wc", wc, wcv)):
        load(name, src, dst)
    left = [remote(kvs.at[i], kvs.at[12 + i], xs.at[0, i], xr.at[0, i], st=xm) for i in range(12)]
    right = [remote(kvs.at[i], kvs.at[36 + i], xs.at[1, i], xr.at[1, i], st=xp) for i in range(12)]
    hop = [remote(kvs.at[12 + i], kvs.at[24 + i], xs.at[2, i], xr.at[2, i], st=xm) for i in range(6)]
    hop += [remote(kvs.at[36 + i], kvs.at[24 + i], xs.at[2, i], xr.at[2, i], st=xp) for i in range(6, 12)]

    loads["wk"].wait()
    loads["wv"].wait()
    for g in range(3):
        for i in ORDER[4 * g:4 * g + 4]:
            loads[i].wait()
        r = sv[4 * g:4 * g + 4].reshape(384, sv.shape[2])
        k = head_normed(dg(r, wkv[...], 1, 0)).astype(BF)
        v = dg(r, wvv[...], 1, 0).astype(BF)
        for u, i in enumerate(ORDER[4 * g:4 * g + 4]):
            kvs[i, :, 0:256] = k[96 * u:96 * u + 96]
            kvs[i, :, 256:512] = v[96 * u:96 * u + 96]
        if g == 0:
            ready()
        for u in range(2):
            left[2 * g + u].start()
            right[6 + 2 * g + u].start()
    for u in range(6):
        left[6 + u].start()
        right[u].start()
    loads["tok"].wait()
    loads["wq"].wait()
    proj = dg(tokv[...], wqv[...], 1, 0)
    qq[0] = (head_normed(proj) * qgain[...]).astype(BF) * BF(0.0625)
    idv[0] = jnp.zeros((8, 128), jnp.int32)
    idv[0, 0:4, 0:8] = ids[...]

    def rows(ref, s, part):
        return ref if s < 3 else ref.at[pl.ds(256 * part, 256), :]

    up, down, up_ids, down_ids = [], [], [], []
    for s in range(4):
        a, b = (8 - s) % 8, 7 - s
        src = qq.at[a]
        up.append(remote(rows(src, s, 0), rows(qq.at[b], s, 0), zs.at[0, s], zr.at[0, s], st=zp))
        up_ids.append(remote(idv.at[a], idv.at[b], ids_s.at[0, s], ids_r.at[0, s], st=zp))
        src = qq.at[s]
        down.append(remote(rows(src, s, 1), rows(qq.at[s + 1], s, 1), zs.at[1, s], zr.at[1, s], st=zm))
        if s < 3:
            down_ids.append(remote(idv.at[s], idv.at[s + 1], ids_s.at[1, s], ids_r.at[1, s], st=zm))

    def z_start(s):
        up[s].start()
        down[s].start()
        up_ids[s].start()
        if s < 3:
            down_ids[s].start()

    def z_wait(s):
        up[s].wait_recv()
        down[s].wait_recv()
        up_ids[s].wait_recv()
        if s < 3:
            down_ids[s].wait_recv()

    z_start(0)
    for name in ("wg", "mq", "mk", "mv"):
        loads[name].wait()
    glow[...] = dg(tokv[...], wgv[...], 1, 0).astype(BF)
    stages = mixer_stages(tokv, mqv, mkv, mvv, wdl, wdu, base, shift, wrl, wru, gain, heads,
                          s_a, s_q, s_ki, s_ri, s_kf, s_rf, s_vs, s_e, s_o)
    next(stages)
    next(stages)
    z_wait(0)
    z_start(1)
    for _ in stages:
        pass
    hspread = Spread(heads, head_all, hs, hr, yp, ym, sib)
    hspread.first(0)
    hspread.first(1)
    for i in range(6):
        left[i].wait_recv()
        hop[i].start()
        right[6 + i].wait_recv()
        hop[6 + i].start()
    z_wait(1)
    z_start(2)
    hspread.second(0)
    hspread.second(1)
    loads["wgu"].wait()
    loads["wm"].wait()
    loads["wc"].wait()
    gate[...] = jax.nn.sigmoid(dg(glow[...], wguv[...], 1, 0))
    z_wait(2)
    z_start(3)
    hspread.third(0)
    hspread.third(1)
    origin = [[lax.rem(y + r, 4) * 2 + (core if c == 0 else 1 - core) for r in range(4)] for c in range(2)]

    def term(buf, w, size, c, r, h):
        at = pl.multiple_of(origin[c][r] * size, size)
        return dg(buf[c, r, h], w[pl.ds(at, size), :], 1, 0)

    rest = [(c, r) for c in range(2) for r in range(4) if (c, r) != (0, 0)]
    at0 = pl.multiple_of(origin[0][0] * 128, 128)
    for h in range(2):
        hspread.arrived(h, 0, 3, 4, 6)
        m = dg(heads[256 * h:256 * h + 256, :], wmv[pl.ds(at0, 128), :], 1, 0)
        for c, r in rest:
            m = m + term(head_all, wmv, 128, c, r, h)
        mixed[256 * h:256 * h + 256, :] = m
    z_wait(3)
    lstv[...] = slot_list(idv[...], z, x)
    put = pltpu.make_async_copy(lstv, lst, in_sem.at[len(loads)])
    put.start()
    put.wait()
    for i in range(6):
        left[6 + i].wait_recv()
        right[i].wait_recv()
    for c in hop:
        c.wait_recv()
    to = {"st_up": zp, "st_down": zm}
    sends = [[remote(msg.at[p, s], box.at[p, s], ps.at[p, s], pr.at[p, s], st=to[way])
              for s in range(len(ds))] for p, (way, _, ds) in enumerate(PIPES)]

    def own(d, h):
        return part[d, 256 * h:256 * h + 256, :], den[8 * d:8 * d + 8, 0:64]

    lane = lax.broadcasted_iota(jnp.int32, (8, 768), 1)
    r128 = lax.broadcasted_iota(jnp.int32, (128, 768), 0)
    diag = lax.broadcasted_iota(jnp.int32, (64, 128), 0) == lax.broadcasted_iota(jnp.int32, (64, 128), 1)

    def attend(d, n):
        u = n % 2
        block = jnp.zeros((8, 768), jnp.int32)
        for r in range(8):
            e = jnp.minimum(jnp.maximum(lst[d, r], 0), 47)
            kd[u, 96 * r:96 * r + 96, :] = kvs[e, :, 0:256]
            vd[u, 96 * r:96 * r + 96, :] = kvs[e, :, 256:512]
            block = jnp.where((lane >= 96 * r) & (lane < 96 * r + 96), lst[d, 64 + r], block)
        block = block[0:1]
        sums = []
        for t in range(4):
            s = slice(128 * t, 128 * t + 128)
            p = jnp.exp(dg(qq[d, s, :], kd[u], 1, 1))
            p = jnp.where(r128 // 64 + (2 * t + 1) == block, p, 0.0)
            part[d, s, :] = dg(p.astype(BF), vd[u], 1, 0)
            total = jnp.sum(p, axis=1, keepdims=True)
            for v in range(2):
                line = jnp.where(diag, total[64 * v:64 * v + 64], 0.0)
                sums.append(jnp.sum(line, axis=0, keepdims=True))
        den[8 * d:8 * d + 8, :] = jnp.concatenate(sums, axis=0)

    def held(p, s):
        line = box[p, s, 256:272, :].astype(F32)[0:8]
        return box[p, s, 0:256, :].astype(F32), line[:, 0:64] + line[:, 64:128]

    def send(p, s):
        _, h, ds = PIPES[p]
        n, d = own(ds[s], h)
        if s:
            sends[p][s - 1].wait_recv()
            n2, d2 = held(p, s - 1)
            n, d = n + n2, d + d2
        msg[p, s, 0:256, :] = n.astype(BF)
        hi = d.astype(BF).astype(F32)
        line = jnp.concatenate([hi, d - hi, jnp.zeros((8, 128), F32)], axis=1)
        msg[p, s, 256:272, :] = jnp.concatenate([line, jnp.zeros((8, 256), F32)], axis=0).astype(BF)
        sends[p][s].start()

    attend(4, 0)
    send(0, 0)
    send(1, 0)
    attend(3, 1)
    send(2, 0)
    attend(5, 0)
    send(3, 0)
    for n, d in enumerate((2, 6, 1, 7, 0)):
        attend(d, n + 1)
    for p in range(4):
        send(p, 1)
    for p in range(4):
        send(p, 2)
    for p in range(2):
        send(p, 3)
    aspread = Spread(att, att_all, as_, ar, yp, ym, sib)
    for h, pipes in ((0, (3, 0)), (1, (2, 1))):
        n, d = own(0, h)
        for p in pipes:
            s = len(PIPES[p][2]) - 1
            sends[p][s].wait_recv()
            n2, d2 = held(p, s)
            n, d = n + n2, d + d2
        inv = jnp.transpose(1.0 / d)
        for b in range(4):
            col = 4 * h + b
            att[256 * h + 64 * b:256 * h + 64 * b + 64, :] = (
                n[64 * b:64 * b + 64] * inv[:, col:col + 1]).astype(BF)
        aspread.first(h)
    at0 = pl.multiple_of(origin[0][0] * 256, 256)
    acc = [dg(att[256 * h:256 * h + 256, :], wcv[pl.ds(at0, 256), :], 1, 0) for h in range(2)]
    aspread.second(0)
    aspread.second(1)
    for h in range(2):
        aspread.arrived(h, 0)
        for c, r in ((0, 3), (0, 1), (1, 0)):
            acc[h] = acc[h] + term(att_all, wcv, 256, c, r, h)
    aspread.third(0)
    aspread.third(1)
    for h in range(2):
        aspread.arrived(h, 3, 4)
        for c, r in ((0, 2), (1, 1), (1, 3)):
            acc[h] = acc[h] + term(att_all, wcv, 256, c, r, h)
    for h in range(2):
        aspread.arrived(h, 6)
        c = acc[h] + term(att_all, wcv, 256, 1, 2, h)
        s = slice(256 * h, 256 * h + 256)
        out[s, :] = (mixed[s, :] + gate[s, :] * c).astype(BF)
    for line in sends:
        for c in line:
            c.wait_send()
    hspread.finish()
    aspread.finish()


    for c in left + right + hop + up + down + up_ids + down_ids:
        c.wait_send()


def local(
    tokens, mix_query, mix_key, mix_value, decay_lower_map, decay_upper_map, decay_base,
    decay_shift, rate_lower_map, rate_upper_map, norm_gain, mix_out, cross_query, score_gain,
    passage_key, passage_value, cross_out, gate_down, gate_up, store, passage_ids,
):
    rows, width = tokens.shape
    sds = jax.ShapeDtypeStruct
    vm = pltpu.VMEM
    dma = pltpu.SemaphoreType.DMA
    f = lambda: vm((rows, 128), F32)
    b = lambda: vm((rows, 128), BF)
    w256 = lambda: vm((width, 256), BF)
    w128 = lambda: vm((width, 128), BF)
    return pl.pallas_call(
        layer_kernel,
        out_shape=sds((rows, 256), BF),
        in_specs=[ANY] * 12 + [VMEM] * 9,
        out_specs=VMEM,
        scratch_shapes=[
            vm((12, 96, width), BF), w256(), w256(), vm((rows, width), BF), w256(), w128(), w128(),
            w128(), w128(), vm(cross_out.shape, BF), vm(mix_out.shape, BF), vm(gate_up.shape, BF),
            vm((48, 96, 512), BF), vm((NZ, rows, 256), BF), vm((8, 8, 128), jnp.int32),
            vm((8, 128), jnp.int32), pltpu.SMEM((8, 128), jnp.int32), b(), b(),
            f(), f(), b(), b(), b(), b(), b(), vm((8, 128), F32), f(),
            vm((2, 768, 256), BF), vm((2, 768, 256), BF), vm((NZ, rows, 256), F32), vm((64, 128), F32),
            vm((4, 4, 272, 256), BF), vm((4, 4, 272, 256), BF), vm((2, 4, 2, 256, 128), BF),
            vm((rows, 256), BF), vm((2, 4, 2, 256, 256), BF), vm((rows, 256), F32), vm((rows, 256), F32),
            dma((24,)), dma((3, 12)), dma((3, 12)), dma((2, 4)), dma((2, 4)), dma((2, 4)), dma((2, 4)),
            dma((4, 4)), dma((4, 4)), dma((2, 7)), dma((2, 7)), dma((2, 7)), dma((2, 7)),
        ],
        compiler_params=params(62, collective_id=0, has_side_effects=True),
        cost_estimate=cost(3e10),
        name="layer",
    )(store, passage_key, passage_value, tokens, cross_query, gate_down, mix_query, mix_key, mix_value,
      cross_out, mix_out, gate_up, score_gain[None], passage_ids.T, decay_lower_map.T, decay_upper_map,
      decay_base[None], decay_shift.T, rate_lower_map.T, rate_upper_map, norm_gain[None])


def solution(mesh):
    placed = (
        P("st", None), P(None, "tp"), P(None, "tp"), P(None, "tp"), P(), P(None, "tp"), P("tp"),
        P("st", "tp"), P(), P(None, "tp"), P("tp"), P(None, "tp"), P(None, "tp"), P("tp"),
        P(None, "tp"), P(None, "tp"), P(None, "tp"), P(), P(None, "tp"), P("st", None, None),
        P("st", None),
    )
    return jax.shard_map(
        local, mesh=mesh, in_specs=placed, out_specs=P("st", "tp"), check_vma=False)
```

```python
import functools
import math

import jax
import jax.numpy as jnp
from jax import lax
from jax.experimental import pallas as pl
from jax.experimental.pallas import tpu as pltpu
from jax.sharding import PartitionSpec as P

F32 = jnp.float32
BF = jnp.bfloat16
NZ, NX = 8, 4
QBLOCK = 64
VMEM = pl.BlockSpec(memory_space=pltpu.VMEM)
MESH = pl.DeviceIdType.MESH
HBM = pl.BlockSpec(memory_space=pltpu.HBM)
SMEM = pl.BlockSpec(memory_space=pltpu.SMEM)
ANY = pl.BlockSpec(memory_space=pl.ANY)


def dg(a, b, ca, cb):
    return lax.dot_general(a, b, (((ca,), (cb,)), ((), ())), preferred_element_type=F32)


def bdot(a, b, ca=1, cb=0):
    return dg(a.astype(BF), b.astype(BF), ca, cb)


def cost(flops):
    return pl.CostEstimate(flops=int(flops), bytes_accessed=int(4e6), transcendentals=0)


def params(mib, **kw):
    return pltpu.CompilerParams(vmem_limit_bytes=mib * 1024 * 1024, **kw)


def head_normed(y):
    return y * lax.rsqrt(jnp.mean(y * y, axis=-1, keepdims=True) + 1e-06)


def exact_sum_dot(left, x, ca, cb, swap):
    hi = x.astype(BF)
    r = x - hi.astype(F32)
    mid = r.astype(BF)
    low = (r - mid.astype(F32)).astype(BF)
    parts = [dg(p, left, ca, cb) if swap else dg(left, p, ca, cb) for p in (hi, mid, low)]
    return parts[0] + parts[1] + parts[2]


def mixer_stages(tok, wq, wk, wv, wdl, wdu, base, shift, wrl, wru, gain, out,
                 s_a, s_q, s_ki, s_ri, s_kf, s_rf, s_vs, s_e, s_o):
    t = tok[...]
    rows = t.shape[0]
    chunks = rows // 64
    lane = lax.broadcasted_iota(jnp.int32, (64, 128), 1)
    row = lax.broadcasted_iota(jnp.int32, (64, 128), 0)
    left = lane < 64
    in_head = jnp.where(left, lane, lane - 64)
    sl = left & (in_head < row)
    sr = jnp.logical_not(left) & (in_head < row)
    upto = in_head <= row
    r2 = lax.broadcasted_iota(jnp.int32, (128, 128), 0)
    l2 = lax.broadcasted_iota(jnp.int32, (128, 128), 1)
    same = (r2 < 64) == (l2 < 64)
    eye = r2 == l2
    ones = jnp.where(same, 1.0, 0.0).astype(BF)
    tri = jnp.where(
        lax.broadcasted_iota(jnp.int32, (64, 64), 1) <= lax.broadcasted_iota(jnp.int32, (64, 64), 0),
        1.0, 0.0).astype(BF)
    q = dg(t, wq[...], 1, 0).astype(BF).astype(F32)
    k = dg(t, wk[...], 1, 0).astype(BF).astype(F32)
    v = dg(t, wv[...], 1, 0).astype(BF).astype(F32)
    low = jnp.tanh(dg(t, wdl[...], 1, 1)).astype(BF)
    spread2 = jnp.where(
        (lax.broadcasted_iota(jnp.int32, (2, 128), 1) < 64)
        == (lax.broadcasted_iota(jnp.int32, (2, 128), 0) == 0), 1.0, 0.0).astype(BF)
    pre = base[...] + dg(low, wdu[...], 1, 0) + exact_sum_dot(spread2, shift[...], 0, 0, True)
    log_fade = jax.nn.sigmoid(pre) * (-math.exp(-0.5))
    rate_low = dg(t, wrl[...], 1, 1).astype(BF)
    rate = jax.nn.sigmoid(dg(rate_low, wru[...], 1, 0))
    unit = k * lax.rsqrt(exact_sum_dot(ones, k * k, 1, 0, True) + 1e-06)
    rate_key = unit * rate
    s_vs[...] = pltpu.roll(v, 64, 1).astype(BF)
    for c in range(chunks):
        s = slice(64 * c, 64 * c + 64)
        f = log_fade[s]
        cumul = exact_sum_dot(tri, f, 1, 0, False)
        end = cumul[63:64]
        ei = jnp.exp(-cumul)
        fo = jnp.exp(end - cumul)
        s_a[s, :] = -unit[s] * jnp.exp(cumul - f)
        s_q[s, :] = q[s] * jnp.exp(cumul)
        s_ki[s, :] = (k[s] * ei).astype(BF)
        s_ri[s, :] = (rate_key[s] * ei).astype(BF)
        s_kf[s, :] = (k[s] * fo).astype(BF)
        s_rf[s, :] = (rate_key[s] * fo).astype(BF)
        s_e[c:c + 1, :] = jnp.exp(end)

    yield
    zb = jnp.zeros((64, 128), BF)
    zf = jnp.zeros((64, 128), F32)

    def only(x, m):
        return jnp.where(m, x, zb if x.dtype == BF else zf)

    right = jnp.logical_not(left)
    cat = jnp.concatenate
    group = 4
    state = jnp.zeros((128, 128), F32)
    for g in range(chunks // group):
        cs = [slice(64 * c, 64 * c + 64) for c in range(g * group, (g + 1) * group)]
        G0, G1, PW, X, VL, VR = [], [], [], [], [], []
        for s in cs:
            a, qq = s_a[s, :].astype(BF), s_q[s, :].astype(BF)
            ki, ri = s_ki[s, :], s_ri[s, :]
            G0.append(dg(cat([only(a, left), only(qq, left)], 0), cat([ri, ki], 0), 1, 1))
            G1.append(dg(cat([only(a, right), only(qq, right)], 0), cat([ki, ri], 0), 1, 1))
        for i, s in enumerate(cs):
            vs = s_vs[s, :]
            VR.append(only(vs, right))
            VL.append(only(vs, left))
            L = cat([only(G0[i][:64], sr), only(G1[i][:64], sl)], 0)
            PW.append(cat([only(G0[i][:64], sl), only(G1[i][:64], sr)], 0))
            a = s_a[s, :]
            X.append(cat([only(a, left), only(a, right)], 0) + bdot(L, cat([VL[i], VR[i]], 0)))
        for it in range(6):
            for i in range(group):
                p16 = PW[i].astype(BF)
                if it < 5:
                    px = dg(p16, cat([p16, X[i].astype(BF)], 1), 1, 0)
                    PW[i] = px[:, :128]
                    X[i] = X[i] + px[:, 128:]
                else:
                    X[i] = X[i] + dg(p16, X[i].astype(BF), 1, 0)
        MM, NN, PC, OO = [], [], [], []
        for i, s in enumerate(cs):
            x16 = X[i].astype(BF)
            h0 = cat([x16[:64], VR[i]], 0)
            h1 = cat([VL[i], x16[64:]], 0)
            y0 = bdot(only(G0[i][64:], upto), h0)
            y1 = bdot(only(G1[i][64:], upto), h1)
            qq = s_q[s, :]
            PC.append(cat([only(y0 + qq, left), only(y1 + qq, right)], 0).astype(BF))
            OO.append(only(y0, right) + only(y1, left))
            kf, rf = s_kf[s, :], s_rf[s, :]
            f = cat([only(rf, left), only(kf, left), only(kf, right), only(rf, right)], 0)
            tr = dg(cat([h0, h1], 0), f, 0, 0)
            e = s_e[g * group + i:g * group + i + 1, :]
            zz = jnp.zeros((128, 128), F32)
            MM.append((jnp.where(same, tr, zz) + jnp.where(eye, e, zz)).astype(BF))
            NN.append(jnp.where(same, zz, tr))
        for i, s in enumerate(cs):
            s16 = state.astype(BF)
            o = dg(PC[i], s16, 1, 1)
            s_o[s, :] = OO[i] + o[:64] + o[64:]
            state = dg(s16, MM[i], 1, 0) + NN[i]
        yield
    o = pltpu.roll(s_o[...], 64, 1)
    centred = o - exact_sum_dot(ones, o, 1, 0, True) * (1.0 / 64)
    spread = exact_sum_dot(ones, centred * centred, 1, 0, True) * (1.0 / 64)
    out[...] = (centred * lax.rsqrt(spread + 0.00064) * gain[...]).astype(BF)


ORDER = (0, 1, 6, 7, 2, 3, 8, 9, 4, 5, 10, 11)


def remote(src, dst, send, recv, **device):
    return pltpu.make_async_remote_copy(
        src_ref=src, dst_ref=dst, send_sem=send, recv_sem=recv, device_id=device,
        device_id_type=MESH)


def meet(peers):
    barrier = pltpu.get_barrier_semaphore()
    for device in peers:
        pl.semaphore_signal(barrier, inc=1, device_id=device, device_id_type=MESH)
    return lambda: pl.semaphore_wait(barrier, len(peers))


def slot_list(ids, z, x):
    row = lax.broadcasted_iota(jnp.int32, (64, 128), 0)
    lane = lax.broadcasted_iota(jnp.int32, (64, 128), 1)
    valid = (row - 8 * (row // 8) < 4) & (lane < 8)
    p = ids.reshape(64, 128).astype(F32)
    plane = jnp.floor((p + 0.5) * (1.0 / 48))
    owner = jnp.floor((p + 0.5) * (1.0 / 12))
    step = owner - 4 * plane - x.astype(F32)
    step = jnp.where(step < 0, step + 4, step)
    slot = step * 12 + p - 12 * owner
    hit = valid & (plane == z.astype(F32))
    m = jnp.where(hit, 1.0, 0.0)
    r1 = lax.broadcasted_iota(jnp.int32, (64, 64), 0)
    c1 = lax.broadcasted_iota(jnp.int32, (64, 64), 1)
    r2 = lax.broadcasted_iota(jnp.int32, (128, 128), 0)
    c2 = lax.broadcasted_iota(jnp.int32, (128, 128), 1)
    near = r1 // 8 == c1 // 8
    above = bdot(jnp.where(near & (c1 < r1), 1.0, 0.0), m)
    column = bdot(jnp.where(near, 1.0, 0.0), m)
    pos = above + bdot(column, jnp.where(r2 < c2, 1.0, 0.0))
    pos = jnp.where(hit, pos, -1.0)
    lanes = lane.astype(F32)
    acc = jnp.zeros((64, 128), F32)
    for b in range(8):
        at = pos[:, b:b + 1]
        acc = acc + jnp.where(at == lanes, slot[:, b:b + 1], 0.0)
        acc = acc + jnp.where((at == lanes - 64) & (at >= 0), b + 1.0, 0.0)
    return jnp.sum(acc.reshape(8, 8, 128), axis=1).astype(jnp.int32)


PIPES = (("st_up", 0, (4, 3, 2, 1)), ("st_down", 1, (4, 5, 6, 7)),
         ("st_up", 1, (3, 2, 1)), ("st_down", 0, (5, 6, 7)))


class Spread:
    def __init__(self, own, buf, send, recv, yp, ym, sib):
        self.copies = []
        for h in range(2):
            s = own.at[pl.ds(256 * h, 256), :]
            links = [(s, buf.at[1, 0, h], sib), (s, buf.at[0, 3, h], yp), (s, buf.at[0, 1, h], ym),
                     (buf.at[0, 3, h], buf.at[1, 3, h], sib), (buf.at[0, 1, h], buf.at[1, 1, h], sib),
                     (buf.at[0, 3, h], buf.at[0, 2, h], yp) if h == 0
                     else (buf.at[0, 1, h], buf.at[0, 2, h], ym),
                     (buf.at[0, 2, h], buf.at[1, 2, h], sib)]
            self.copies.append([
                remote(a, b, send.at[h, k], recv.at[h, k], tp=to) for k, (a, b, to) in enumerate(links)])

    def first(self, h):
        c = self.copies[h]
        for k in ((1, 2, 0) if h == 0 else (2, 1, 0)):
            c[k].start()

    def second(self, h):
        c = self.copies[h]
        if h == 0:
            c[1].wait_recv()
            c[5].start()
            c[3].start()
            c[2].wait_recv()
            c[4].start()
        else:
            c[2].wait_recv()
            c[5].start()
            c[4].start()
            c[1].wait_recv()
            c[3].start()

    def third(self, h):
        self.copies[h][5].wait_recv()
        self.copies[h][6].start()

    def arrived(self, h, *which):
        for k in which:
            self.copies[h][k].wait_recv()


def layer_kernel(store, wk, wv, tok, wq, wg, mq, mk, mv, wc, wm, wgu, qgain, ids, wdl, wdu, base, shift, wrl,
                 wru, gain, out,
                 sv, wkv, wvv, tokv, wqv, wgv, mqv, mkv, mvv, wcv, wmv, wguv, ks, vs0, vs1, qq, idv, lstv, lst,
                 glow, heads, s_a, s_q, s_ki, s_ri, s_kf, s_rf, s_vs, s_e, s_o,
                 kd, vd, pbuf, part, den, msg, box, head_all, att, att_all, gate, mixed,
                 in_sem, k_s, k_r, kh_s, kh_r, v_s, v_r, vh_s, vh_r, zs, zr, ids_s, ids_r, ps, pr, sp_s, sp_r):
    vs = (vs0, vs1)
    st, tp = lax.axis_index("st"), lax.axis_index("tp")
    z, x = st // NX, lax.rem(st, NX)
    y, core = tp // 2, lax.rem(tp, 2)
    xp = z * NX + lax.rem(x + 1, NX)
    xm = z * NX + lax.rem(x + NX - 1, NX)
    zp = lax.rem(z + 1, NZ) * NX + x
    zm = lax.rem(z + NZ - 1, NZ) * NX + x
    yp = lax.rem(y + 1, 4) * 2 + core
    ym = lax.rem(y + 3, 4) * 2 + core
    sib = y * 2 + 1 - core
    ready = meet([{"st": xp}, {"st": xm}, {"st": zp}, {"st": zm}, {"tp": yp}, {"tp": ym}, {"tp": sib}])
    loads = {}

    def load(name, src, dst):
        loads[name] = pltpu.make_async_copy(src, dst, in_sem.at[len(loads)])
        loads[name].start()

    load("tok", tok, tokv)
    load("wq", wq, wqv)
    load("wk", wk, wkv)
    load("wv", wv, wvv)
    for p, i in enumerate(ORDER):
        load(i, store.at[i], sv.at[p])
    for name, src, dst in (("wg", wg, wgv), ("mq", mq, mqv), ("mk", mk, mkv), ("mv", mv, mvv),
                           ("wm", wm, wmv), ("wgu", wgu, wguv), ("wc", wc, wcv)):
        load(name, src, dst)

    left = [remote(ks.at[i], ks.at[12 + i], k_s.at[0, i], k_r.at[0, i], st=xm) for i in range(12)]
    right = [remote(ks.at[i], ks.at[36 + i], k_s.at[1, i], k_r.at[1, i], st=xp) for i in range(12)]

    def six(ref, at):
        return ref.at[pl.ds(at, 6)]

    khop = [remote(six(ks, 12), six(ks, 24), kh_s.at[0], kh_r.at[0], st=xm),
            remote(six(ks, 42), six(ks, 30), kh_s.at[1], kh_r.at[1], st=xp)]
    vleft = [[remote(six(vs[c], 6 * i), six(vs[c], 12 + 6 * i), v_s.at[c, 0, i], v_r.at[c, 0, i], st=xm)
              for i in range(2)] for c in range(2)]
    vright = [[remote(six(vs[c], 6 * i), six(vs[c], 36 + 6 * i), v_s.at[c, 1, i], v_r.at[c, 1, i], st=xp)
               for i in range(2)] for c in range(2)]
    vhop = [[remote(six(vs[c], 12), six(vs[c], 24), vh_s.at[c, 0], vh_r.at[c, 0], st=xm),
             remote(six(vs[c], 42), six(vs[c], 30), vh_s.at[c, 1], vh_r.at[c, 1], st=xp)]
            for c in range(2)]

    def v_start(c):
        vleft[c][0].start()
        vright[c][1].start()
        vleft[c][1].start()
        vright[c][0].start()

    def v_hop(c):
        vleft[c][0].wait_recv()
        vhop[c][0].start()
        vright[c][1].wait_recv()
        vhop[c][1].start()

    def v_wait(c):
        vleft[c][1].wait_recv()
        vright[c][0].wait_recv()
        vhop[c][0].wait_recv()
        vhop[c][1].wait_recv()

    def rows(ref, s, half):
        return ref if s < 3 else ref.at[pl.ds(256 * half, 256), :]

    up, down, id_steps = [], [], []
    for s in range(4):
        a, b = (8 - s) % 8, 7 - s
        up.append(remote(rows(qq.at[a], s, 0), rows(qq.at[b], s, 0), zs.at[0, s], zr.at[0, s], st=zp))
        down.append(remote(rows(qq.at[s], s, 1), rows(qq.at[s + 1], s, 1), zs.at[1, s], zr.at[1, s], st=zm))
        steps = [remote(idv.at[a], idv.at[b], ids_s.at[0, s], ids_r.at[0, s], st=zp)]
        if s < 3:
            steps.append(remote(idv.at[s], idv.at[s + 1], ids_s.at[1, s], ids_r.at[1, s], st=zm))
        id_steps.append(steps)

    def z_start(s):
        up[s].start()
        down[s].start()

    def z_wait(s):
        up[s].wait_recv()
        down[s].wait_recv()

    def ids_start(s):
        for c in id_steps[s]:
            c.start()

    def ids_wait(s):
        for c in id_steps[s]:
            c.wait_recv()

    idv[0] = jnp.zeros((8, 128), jnp.int32)
    idv[0, 0:4, 0:8] = ids[...]
    loads["tok"].wait()
    loads["wq"].wait()
    proj = dg(tokv[...], wqv[...], 1, 0)
    qq[0] = (head_normed(proj) * qgain[...]).astype(BF) * BF(0.0625)
    ready()
    ids_start(0)
    z_start(0)
    loads["wk"].wait()
    loads["wv"].wait()
    for g in range(3):
        for i in ORDER[4 * g:4 * g + 4]:
            loads[i].wait()
        r = sv[4 * g:4 * g + 4].reshape(384, sv.shape[2])
        k = head_normed(dg(r, wkv[...], 1, 0)).astype(BF)
        for u, i in enumerate(ORDER[4 * g:4 * g + 4]):
            ks[i] = k[96 * u:96 * u + 96]
        for u in range(2):
            left[2 * g + u].start()
            right[6 + 2 * g + u].start()
    for u in range(6):
        left[6 + u].start()
        right[u].start()
    ids_wait(0)
    ids_start(1)
    for g in range(3):
        v = dg(sv[4 * g:4 * g + 4].reshape(384, sv.shape[2]), wvv[...], 1, 0).astype(BF)
        for u, i in enumerate(ORDER[4 * g:4 * g + 4]):
            vs0[i] = v[96 * u:96 * u + 96, 0:128]
            vs1[i] = v[96 * u:96 * u + 96, 128:256]
    ids_wait(1)
    ids_start(2)
    for name in ("wg", "mq", "mk", "mv"):
        loads[name].wait()
    glow[...] = dg(tokv[...], wgv[...], 1, 0).astype(BF)
    stages = mixer_stages(tokv, mqv, mkv, mvv, wdl, wdu, base, shift, wrl, wru, gain, heads,
                          s_a, s_q, s_ki, s_ri, s_kf, s_rf, s_vs, s_e, s_o)
    next(stages)
    z_wait(0)
    z_start(1)
    ids_wait(2)
    ids_start(3)
    next(stages)
    for i in range(6):
        left[i].wait_recv()
    khop[0].start()
    for i in range(6):
        right[6 + i].wait_recv()
    khop[1].start()
    v_start(0)
    for _ in stages:
        pass
    ids_wait(3)
    lstv[...] = slot_list(idv[...], z, x)
    put = pltpu.make_async_copy(lstv, lst, in_sem.at[len(loads)])
    put.start()
    z_wait(1)
    z_start(2)
    hspread = Spread(heads, head_all, sp_s.at[0], sp_r.at[0], yp, ym, sib)
    hspread.first(0)
    hspread.first(1)
    loads["wgu"].wait()
    loads["wm"].wait()
    loads["wc"].wait()
    gate[...] = jax.nn.sigmoid(dg(glow[...], wguv[...], 1, 0))
    put.wait()

    lane = lax.broadcasted_iota(jnp.int32, (8, 768), 1)
    r128 = lax.broadcasted_iota(jnp.int32, (128, 768), 0)
    diag = lax.broadcasted_iota(jnp.int32, (64, 128), 0) == lax.broadcasted_iota(jnp.int32, (64, 128), 1)

    def slot(d, r):
        return jnp.minimum(jnp.maximum(lst[d, r], 0), 47)

    def scores(d, u):
        block = jnp.zeros((8, 768), jnp.int32)
        for r in range(8):
            kd[u, 96 * r:96 * r + 96, :] = ks[slot(d, r)]
            block = jnp.where((lane >= 96 * r) & (lane < 96 * r + 96), lst[d, 64 + r], block)
        block = block[0:1]
        sums = []
        for t in range(4):
            s = slice(128 * t, 128 * t + 128)
            p = jnp.exp(dg(qq[d, s, :], kd[u], 1, 1))
            p = jnp.where(r128 // 64 + (2 * t + 1) == block, p, 0.0)
            pbuf[d, s, :] = p.astype(BF)
            total = jnp.sum(p, axis=1, keepdims=True)
            for v in range(2):
                line = jnp.where(diag, total[64 * v:64 * v + 64], 0.0)
                sums.append(jnp.sum(line, axis=0, keepdims=True))
        den[8 * d:8 * d + 8, :] = jnp.concatenate(sums, axis=0)

    def values(c, d, u):
        for r in range(8):
            vd[u, 96 * r:96 * r + 96, :] = vs[c][slot(d, r)]
        part[c, d] = dg(pbuf[d], vd[u], 1, 0)

    for i in range(6):
        left[6 + i].wait_recv()
        right[i].wait_recv()
    khop[0].wait_recv()
    khop[1].wait_recv()
    for n, d in enumerate((0, 1, 7, 2, 6)):
        scores(d, n % 2)
    z_wait(2)
    z_start(3)
    scores(3, 1)
    scores(5, 0)
    v_hop(0)
    v_start(1)
    hspread.second(0)
    hspread.second(1)
    origin = [[lax.rem(y + r, 4) * 2 + (core if c == 0 else 1 - core) for r in range(4)] for c in range(2)]
    rest = [(c, r) for c in range(2) for r in range(4) if (c, r) != (0, 0)]

    def weight(w, size, c, r, shift_rows):
        at = pl.multiple_of(origin[c][r] * size + shift_rows, 128)
        return w[pl.ds(at, 128), :]

    hspread.third(0)
    hspread.third(1)
    z_wait(3)
    scores(4, 1)
    for h in range(2):
        hspread.arrived(h, 0, 3, 4, 6)
        m = dg(heads[256 * h:256 * h + 256, :], weight(wmv, 128, 0, 0, 0), 1, 0)
        for c, r in rest:
            m = m + dg(head_all[c, r, h], weight(wmv, 128, c, r, 0), 1, 0)
        mixed[256 * h:256 * h + 256, :] = m

    to = {"st_up": zp, "st_down": zm}

    def box_rows(ref, c, p, s):
        return ref.at[c, p, s] if c == 0 else ref.at[c, p, s, pl.ds(0, 256), :]

    sends = [[[remote(box_rows(msg, c, p, s), box_rows(box, c, p, s), ps.at[c, p, s], pr.at[c, p, s], st=to[way])
               for s in range(len(ds))] for p, (way, _, ds) in enumerate(PIPES)] for c in range(2)]

    def own(c, d, h):
        return part[c, d, 256 * h:256 * h + 256, :], den[8 * d:8 * d + 8, 0:64]

    def held(c, p, s):
        n = box[c, p, s, 0:256, :].astype(F32)
        if c == 1:
            return n, 0.0
        line = box[c, p, s, 256:272, :].astype(F32)[0:8]
        return n, line[:, 0:64] + line[:, 64:128]

    def send(c, p, s):
        _, h, ds = PIPES[p]
        n, d = own(c, ds[s], h)
        if s:
            sends[c][p][s - 1].wait_recv()
            n2, d2 = held(c, p, s - 1)
            n, d = n + n2, d + d2
        msg[c, p, s, 0:256, :] = n.astype(BF)
        if c == 0:
            hi = d.astype(BF).astype(F32)
            line = jnp.concatenate([hi, d - hi], axis=1)
            msg[c, p, s, 256:272, :] = jnp.concatenate([line, jnp.zeros((8, 128), F32)], axis=0).astype(BF)
        sends[c][p][s].start()

    inverse = [None, None]
    spread = [Spread(att.at[c], att_all.at[c], sp_s.at[1 + c], sp_r.at[1 + c], yp, ym, sib) for c in range(2)]

    def settle(c):
        for h, pipes in ((0, (3, 0)), (1, (2, 1))):
            n, d = own(c, 0, h)
            for p in pipes:
                s = len(PIPES[p][2]) - 1
                sends[c][p][s].wait_recv()
                n2, d2 = held(c, p, s)
                n, d = n + n2, d + d2
            if c == 0:
                inverse[h] = jnp.transpose(1.0 / d)
            for b in range(4):
                col = 4 * h + b
                att[c, 256 * h + 64 * b:256 * h + 64 * b + 64, :] = (
                    n[64 * b:64 * b + 64] * inverse[h][:, col:col + 1]).astype(BF)
            spread[c].first(h)

    def begin(c):
        values(c, 4, 0)
        send(c, 0, 0)
        send(c, 1, 0)
        values(c, 3, 1)
        send(c, 2, 0)
        values(c, 5, 0)
        send(c, 3, 0)
        for n, d in enumerate((2, 6, 1, 7, 0)):
            values(c, d, (n + 1) % 2)

    def step(c, s):
        for p in range(4):
            if s < len(PIPES[p][2]):
                send(c, p, s)

    def add(acc, c, h, which):
        for q, r in which:
            acc = acc + dg(att_all[c, q, r, h], weight(wcv, 256, q, r, 128 * c), 1, 0)
        return acc

    v_wait(0)
    begin(0)
    v_hop(1)
    step(0, 1)
    step(0, 2)
    v_wait(1)
    begin(1)
    step(0, 3)
    step(1, 1)
    settle(0)
    step(1, 2)
    spread[0].second(0)
    spread[0].second(1)
    step(1, 3)
    spread[0].third(0)
    spread[0].third(1)
    acc = []
    for h in range(2):
        a = dg(att[0, 256 * h:256 * h + 256, :], weight(wcv, 256, 0, 0, 0), 1, 0)
        spread[0].arrived(h, 0, 3, 4, 6)
        acc.append(add(a, 0, h, rest))
    settle(1)
    for h in range(2):
        acc[h] = acc[h] + dg(att[1, 256 * h:256 * h + 256, :], weight(wcv, 256, 0, 0, 128), 1, 0)
    spread[1].second(0)
    spread[1].second(1)
    for h in range(2):
        spread[1].arrived(h, 0)
        acc[h] = add(acc[h], 1, h, ((0, 3), (0, 1), (1, 0)))
    spread[1].third(0)
    spread[1].third(1)
    for h in range(2):
        spread[1].arrived(h, 3, 4)
        acc[h] = add(acc[h], 1, h, ((0, 2), (1, 1), (1, 3)))
    for h in range(2):
        spread[1].arrived(h, 6)
        c = add(acc[h], 1, h, ((1, 2),))
        s = slice(256 * h, 256 * h + 256)
        out[s, :] = (mixed[s, :] + gate[s, :] * c).astype(BF)
    for group in (left, right, khop, *vleft, *vright, *vhop, up, down, *id_steps,
                  *sends[0], *sends[1], *(p for sp in (hspread, *spread) for p in sp.copies)):
        for c in group:
            c.wait_send()


def local(
    tokens, mix_query, mix_key, mix_value, decay_lower_map, decay_upper_map, decay_base,
    decay_shift, rate_lower_map, rate_upper_map, norm_gain, mix_out, cross_query, score_gain,
    passage_key, passage_value, cross_out, gate_down, gate_up, store, passage_ids,
):
    rows, width = tokens.shape
    sds = jax.ShapeDtypeStruct
    vm = pltpu.VMEM
    dma = pltpu.SemaphoreType.DMA
    f = lambda: vm((rows, 128), F32)
    b = lambda: vm((rows, 128), BF)
    w256 = lambda: vm((width, 256), BF)
    w128 = lambda: vm((width, 128), BF)
    return pl.pallas_call(
        layer_kernel,
        out_shape=sds((rows, 256), BF),
        in_specs=[ANY] * 12 + [VMEM] * 9,
        out_specs=VMEM,
        scratch_shapes=[
            vm((12, 96, width), BF), w256(), w256(), vm((rows, width), BF), w256(), w128(), w128(),
            w128(), w128(), vm(cross_out.shape, BF), vm(mix_out.shape, BF), vm(gate_up.shape, BF),
            vm((48, 96, 256), BF), vm((48, 96, 128), BF), vm((48, 96, 128), BF), vm((NZ, rows, 256), BF),
            vm((8, 8, 128), jnp.int32), vm((8, 128), jnp.int32), pltpu.SMEM((8, 128), jnp.int32), b(), b(),
            f(), f(), b(), b(), b(), b(), b(), vm((8, 128), F32), f(),
            vm((2, 768, 256), BF), vm((2, 768, 128), BF), vm((NZ, rows, 768), BF),
            vm((2, NZ, rows, 128), F32), vm((64, 128), F32),
            vm((2, 4, 4, 272, 128), BF), vm((2, 4, 4, 272, 128), BF), vm((2, 4, 2, 256, 128), BF),
            vm((2, rows, 128), BF), vm((2, 2, 4, 2, 256, 128), BF), vm((rows, 256), F32), vm((rows, 256), F32),
            dma((24,)), dma((2, 12)), dma((2, 12)), dma((2,)), dma((2,)), dma((2, 2, 2)), dma((2, 2, 2)),
            dma((2, 2)), dma((2, 2)), dma((2, 4)), dma((2, 4)), dma((2, 4)), dma((2, 4)),
            dma((2, 4, 4)), dma((2, 4, 4)), dma((3, 2, 7)), dma((3, 2, 7)),
        ],
        compiler_params=params(62, collective_id=0, has_side_effects=True),
        cost_estimate=cost(3e10),
        name="layer",
    )(store, passage_key, passage_value, tokens, cross_query, gate_down, mix_query, mix_key, mix_value,
      cross_out, mix_out, gate_up, score_gain[None], passage_ids.T, decay_lower_map.T, decay_upper_map,
      decay_base[None], decay_shift.T, rate_lower_map.T, rate_upper_map, norm_gain[None])


def solution(mesh):
    placed = (
        P("st", None), P(None, "tp"), P(None, "tp"), P(None, "tp"), P(), P(None, "tp"), P("tp"),
        P("st", "tp"), P(), P(None, "tp"), P("tp"), P(None, "tp"), P(None, "tp"), P("tp"),
        P(None, "tp"), P(None, "tp"), P(None, "tp"), P(), P(None, "tp"), P("st", None, None),
        P("st", None),
    )
    return jax.shard_map(
        local, mesh=mesh, in_specs=placed, out_specs=P("st", "tp"), check_vma=False)
```

```python
import functools
import math

import jax
import jax.numpy as jnp
from jax import lax
from jax.experimental import pallas as pl
from jax.experimental.pallas import tpu as pltpu
from jax.sharding import PartitionSpec as P

F32 = jnp.float32
BF = jnp.bfloat16
NZ, NX = 8, 4
QBLOCK = 64
VMEM = pl.BlockSpec(memory_space=pltpu.VMEM)
MESH = pl.DeviceIdType.MESH
HBM = pl.BlockSpec(memory_space=pltpu.HBM)
SMEM = pl.BlockSpec(memory_space=pltpu.SMEM)
ANY = pl.BlockSpec(memory_space=pl.ANY)


def dg(a, b, ca, cb):
    return lax.dot_general(a, b, (((ca,), (cb,)), ((), ())), preferred_element_type=F32)


def bdot(a, b, ca=1, cb=0):
    return dg(a.astype(BF), b.astype(BF), ca, cb)


def cost(flops):
    return pl.CostEstimate(flops=int(flops), bytes_accessed=int(4e6), transcendentals=0)


def params(mib, **kw):
    return pltpu.CompilerParams(vmem_limit_bytes=mib * 1024 * 1024, **kw)


def head_normed(y):
    return y * lax.rsqrt(jnp.mean(y * y, axis=-1, keepdims=True) + 1e-06)


def exact_sum_dot(left, x, ca, cb, swap):
    hi = x.astype(BF)
    r = x - hi.astype(F32)
    mid = r.astype(BF)
    low = (r - mid.astype(F32)).astype(BF)
    parts = [dg(p, left, ca, cb) if swap else dg(left, p, ca, cb) for p in (hi, mid, low)]
    return parts[0] + parts[1] + parts[2]


def mixer_stages(tok, wq, wk, wv, wdl, wdu, base, shift, wrl, wru, gain, out,
                 s_a, s_q, s_ki, s_ri, s_kf, s_rf, s_vs, s_e, s_o):
    t = tok[...]
    rows = t.shape[0]
    chunks = rows // 64
    lane = lax.broadcasted_iota(jnp.int32, (64, 128), 1)
    row = lax.broadcasted_iota(jnp.int32, (64, 128), 0)
    left = lane < 64
    in_head = jnp.where(left, lane, lane - 64)
    sl = left & (in_head < row)
    sr = jnp.logical_not(left) & (in_head < row)
    upto = in_head <= row
    r2 = lax.broadcasted_iota(jnp.int32, (128, 128), 0)
    l2 = lax.broadcasted_iota(jnp.int32, (128, 128), 1)
    same = (r2 < 64) == (l2 < 64)
    eye = r2 == l2
    ones = jnp.where(same, 1.0, 0.0).astype(BF)
    tri = jnp.where(
        lax.broadcasted_iota(jnp.int32, (64, 64), 1) <= lax.broadcasted_iota(jnp.int32, (64, 64), 0),
        1.0, 0.0).astype(BF)
    q = dg(t, wq[...], 1, 0).astype(BF).astype(F32)
    k = dg(t, wk[...], 1, 0).astype(BF).astype(F32)
    v = dg(t, wv[...], 1, 0).astype(BF).astype(F32)
    low = jnp.tanh(dg(t, wdl[...], 1, 1)).astype(BF)
    spread2 = jnp.where(
        (lax.broadcasted_iota(jnp.int32, (2, 128), 1) < 64)
        == (lax.broadcasted_iota(jnp.int32, (2, 128), 0) == 0), 1.0, 0.0).astype(BF)
    pre = base[...] + dg(low, wdu[...], 1, 0) + exact_sum_dot(spread2, shift[...], 0, 0, True)
    log_fade = jax.nn.sigmoid(pre) * (-math.exp(-0.5))
    rate_low = dg(t, wrl[...], 1, 1).astype(BF)
    rate = jax.nn.sigmoid(dg(rate_low, wru[...], 1, 0))
    yield
    unit = k * lax.rsqrt(exact_sum_dot(ones, k * k, 1, 0, True) + 1e-06)
    rate_key = unit * rate
    s_vs[...] = pltpu.roll(v, 64, 1).astype(BF)
    for c in range(chunks):
        s = slice(64 * c, 64 * c + 64)
        f = log_fade[s]
        cumul = exact_sum_dot(tri, f, 1, 0, False)
        end = cumul[63:64]
        ei = jnp.exp(-cumul)
        fo = jnp.exp(end - cumul)
        s_a[s, :] = -unit[s] * jnp.exp(cumul - f)
        s_q[s, :] = q[s] * jnp.exp(cumul)
        s_ki[s, :] = (k[s] * ei).astype(BF)
        s_ri[s, :] = (rate_key[s] * ei).astype(BF)
        s_kf[s, :] = (k[s] * fo).astype(BF)
        s_rf[s, :] = (rate_key[s] * fo).astype(BF)
        s_e[c:c + 1, :] = jnp.exp(end)

    yield
    zb = jnp.zeros((64, 128), BF)
    zf = jnp.zeros((64, 128), F32)

    def only(x, m):
        return jnp.where(m, x, zb if x.dtype == BF else zf)

    right = jnp.logical_not(left)
    cat = jnp.concatenate
    group = 4
    state = jnp.zeros((128, 128), F32)
    for g in range(chunks // group):
        cs = [slice(64 * c, 64 * c + 64) for c in range(g * group, (g + 1) * group)]
        G0, G1, PW, X, VL, VR = [], [], [], [], [], []
        for s in cs:
            a, qq = s_a[s, :].astype(BF), s_q[s, :].astype(BF)
            ki, ri = s_ki[s, :], s_ri[s, :]
            G0.append(dg(cat([only(a, left), only(qq, left)], 0), cat([ri, ki], 0), 1, 1))
            G1.append(dg(cat([only(a, right), only(qq, right)], 0), cat([ki, ri], 0), 1, 1))
        for i, s in enumerate(cs):
            vs = s_vs[s, :]
            VR.append(only(vs, right))
            VL.append(only(vs, left))
            L = cat([only(G0[i][:64], sr), only(G1[i][:64], sl)], 0)
            PW.append(cat([only(G0[i][:64], sl), only(G1[i][:64], sr)], 0))
            a = s_a[s, :]
            X.append(cat([only(a, left), only(a, right)], 0) + bdot(L, cat([VL[i], VR[i]], 0)))
        for it in range(6):
            for i in range(group):
                p16 = PW[i].astype(BF)
                if it < 5:
                    px = dg(p16, cat([p16, X[i].astype(BF)], 1), 1, 0)
                    PW[i] = px[:, :128]
                    X[i] = X[i] + px[:, 128:]
                else:
                    X[i] = X[i] + dg(p16, X[i].astype(BF), 1, 0)
        MM, NN, PC, OO = [], [], [], []
        for i, s in enumerate(cs):
            x16 = X[i].astype(BF)
            h0 = cat([x16[:64], VR[i]], 0)
            h1 = cat([VL[i], x16[64:]], 0)
            y0 = bdot(only(G0[i][64:], upto), h0)
            y1 = bdot(only(G1[i][64:], upto), h1)
            qq = s_q[s, :]
            PC.append(cat([only(y0 + qq, left), only(y1 + qq, right)], 0).astype(BF))
            OO.append(only(y0, right) + only(y1, left))
            kf, rf = s_kf[s, :], s_rf[s, :]
            f = cat([only(rf, left), only(kf, left), only(kf, right), only(rf, right)], 0)
            tr = dg(cat([h0, h1], 0), f, 0, 0)
            e = s_e[g * group + i:g * group + i + 1, :]
            zz = jnp.zeros((128, 128), F32)
            MM.append((jnp.where(same, tr, zz) + jnp.where(eye, e, zz)).astype(BF))
            NN.append(jnp.where(same, zz, tr))
        for i, s in enumerate(cs):
            s16 = state.astype(BF)
            o = dg(PC[i], s16, 1, 1)
            s_o[s, :] = OO[i] + o[:64] + o[64:]
            state = dg(s16, MM[i], 1, 0) + NN[i]
        yield
    o = pltpu.roll(s_o[...], 64, 1)
    centred = o - exact_sum_dot(ones, o, 1, 0, True) * (1.0 / 64)
    spread = exact_sum_dot(ones, centred * centred, 1, 0, True) * (1.0 / 64)
    out[...] = (centred * lax.rsqrt(spread + 0.00064) * gain[...]).astype(BF)


ORDER = (0, 1, 6, 7, 2, 3, 8, 9, 4, 5, 10, 11)


def remote(src, dst, send, recv, **device):
    return pltpu.make_async_remote_copy(
        src_ref=src, dst_ref=dst, send_sem=send, recv_sem=recv, device_id=device,
        device_id_type=MESH)


def meet(peers):
    barrier = pltpu.get_barrier_semaphore()
    for device in peers:
        pl.semaphore_signal(barrier, inc=1, device_id=device, device_id_type=MESH)
    return lambda: pl.semaphore_wait(barrier, len(peers))


def slot_list(ids, z, x):
    row = lax.broadcasted_iota(jnp.int32, (64, 128), 0)
    lane = lax.broadcasted_iota(jnp.int32, (64, 128), 1)
    valid = (row - 8 * (row // 8) < 4) & (lane < 8)
    p = ids.reshape(64, 128).astype(F32)
    plane = jnp.floor((p + 0.5) * (1.0 / 48))
    owner = jnp.floor((p + 0.5) * (1.0 / 12))
    step = owner - 4 * plane - x.astype(F32)
    step = jnp.where(step < 0, step + 4, step)
    slot = step * 12 + p - 12 * owner
    hit = valid & (plane == z.astype(F32))
    m = jnp.where(hit, 1.0, 0.0)
    r1 = lax.broadcasted_iota(jnp.int32, (64, 64), 0)
    c1 = lax.broadcasted_iota(jnp.int32, (64, 64), 1)
    r2 = lax.broadcasted_iota(jnp.int32, (128, 128), 0)
    c2 = lax.broadcasted_iota(jnp.int32, (128, 128), 1)
    near = r1 // 8 == c1 // 8
    above = bdot(jnp.where(near & (c1 < r1), 1.0, 0.0), m)
    column = bdot(jnp.where(near, 1.0, 0.0), m)
    pos = above + bdot(column, jnp.where(r2 < c2, 1.0, 0.0))
    pos = jnp.where(hit, pos, -1.0)
    lanes = lane.astype(F32)
    acc = jnp.zeros((64, 128), F32)
    for b in range(8):
        at = pos[:, b:b + 1]
        acc = acc + jnp.where(at == lanes, slot[:, b:b + 1], 0.0)
        acc = acc + jnp.where((at == lanes - 64) & (at >= 0), b + 1.0, 0.0)
    return jnp.sum(acc.reshape(8, 8, 128), axis=1).astype(jnp.int32)


PIPES = (("st_up", 0, (4, 3, 2, 1)), ("st_down", 1, (4, 5, 6, 7)),
         ("st_up", 1, (3, 2, 1)), ("st_down", 0, (5, 6, 7)))


class Spread:
    def __init__(self, own, buf, send, recv, yp, ym, sib):
        self.copies = []
        for h in range(2):
            s = own.at[pl.ds(256 * h, 256), :]
            links = [(s, buf.at[1, 0, h], sib), (s, buf.at[0, 3, h], yp), (s, buf.at[0, 1, h], ym),
                     (buf.at[0, 3, h], buf.at[1, 3, h], sib), (buf.at[0, 1, h], buf.at[1, 1, h], sib),
                     (buf.at[0, 3, h], buf.at[0, 2, h], yp) if h == 0
                     else (buf.at[0, 1, h], buf.at[0, 2, h], ym),
                     (buf.at[0, 2, h], buf.at[1, 2, h], sib)]
            self.copies.append([
                remote(a, b, send.at[h, k], recv.at[h, k], tp=to) for k, (a, b, to) in enumerate(links)])

    def first(self, h):
        c = self.copies[h]
        for k in ((1, 2, 0) if h == 0 else (2, 1, 0)):
            c[k].start()

    def second(self, h):
        c = self.copies[h]
        if h == 0:
            c[1].wait_recv()
            c[5].start()
            c[3].start()
            c[2].wait_recv()
            c[4].start()
        else:
            c[2].wait_recv()
            c[5].start()
            c[4].start()
            c[1].wait_recv()
            c[3].start()

    def third(self, h):
        self.copies[h][5].wait_recv()
        self.copies[h][6].start()

    def arrived(self, h, *which):
        for k in which:
            self.copies[h][k].wait_recv()


def layer_kernel(store, wk, wv, tok, wq, wg, mq, mk, mv, wc, wm, wgu, qgain, ids, wdl, wdu, base, shift, wrl,
                 wru, gain, out,
                 sv, wkv, wvv, tokv, wqv, wgv, mqv, mkv, mvv, wcv, wmv, wguv, ks, vs0, vs1, qq, idv, lstv, lst,
                 glow, heads, s_a, s_q, s_ki, s_ri, s_kf, s_rf, s_vs, s_e, s_o,
                 kd, vd, pbuf, part, den, msg, box, head_all, att, att_all, gate, mixed,
                 in_sem, k_s, k_r, kh_s, kh_r, v_s, v_r, vh_s, vh_r, zs, zr, ids_s, ids_r, ps, pr, sp_s, sp_r):
    vs = (vs0, vs1)
    st, tp = lax.axis_index("st"), lax.axis_index("tp")
    z, x = st // NX, lax.rem(st, NX)
    y, core = tp // 2, lax.rem(tp, 2)
    xp = z * NX + lax.rem(x + 1, NX)
    xm = z * NX + lax.rem(x + NX - 1, NX)
    zp = lax.rem(z + 1, NZ) * NX + x
    zm = lax.rem(z + NZ - 1, NZ) * NX + x
    yp = lax.rem(y + 1, 4) * 2 + core
    ym = lax.rem(y + 3, 4) * 2 + core
    sib = y * 2 + 1 - core
    ready = meet([{"st": xp}, {"st": xm}, {"st": zp}, {"st": zm}, {"tp": yp}, {"tp": ym}, {"tp": sib}])
    loads = {}

    def load(name, src, dst):
        loads[name] = pltpu.make_async_copy(src, dst, in_sem.at[len(loads)])
        loads[name].start()

    load("tok", tok, tokv)
    load("wq", wq, wqv)
    load("wk", wk, wkv)
    load("wv", wv, wvv)
    for p, i in enumerate(ORDER):
        load(i, store.at[i], sv.at[p])
    for name, src, dst in (("wg", wg, wgv), ("mq", mq, mqv), ("mk", mk, mkv), ("mv", mv, mvv),
                           ("wm", wm, wmv), ("wgu", wgu, wguv), ("wc", wc, wcv)):
        load(name, src, dst)

    def six(ref, at, n=6):
        return ref.at[pl.ds(at, n)]

    left = [remote(six(ks, a, n), six(ks, 12 + a, n), k_s.at[0, i], k_r.at[0, i], st=xm)
            for i, (a, n) in enumerate(((0, 2), (2, 2), (4, 2), (6, 6)))]
    right = [remote(six(ks, a, n), six(ks, 36 + a, n), k_s.at[1, i], k_r.at[1, i], st=xp)
             for i, (a, n) in enumerate(((6, 2), (8, 2), (10, 2), (0, 6)))]

    khop = [remote(six(ks, 12), six(ks, 24), kh_s.at[0], kh_r.at[0], st=xm),
            remote(six(ks, 42), six(ks, 30), kh_s.at[1], kh_r.at[1], st=xp)]
    vleft = [[remote(six(vs[c], 6 * i), six(vs[c], 12 + 6 * i), v_s.at[c, 0, i], v_r.at[c, 0, i], st=xm)
              for i in range(2)] for c in range(2)]
    vright = [[remote(six(vs[c], 6 * i), six(vs[c], 36 + 6 * i), v_s.at[c, 1, i], v_r.at[c, 1, i], st=xp)
               for i in range(2)] for c in range(2)]
    vhop = [[remote(six(vs[c], 12), six(vs[c], 24), vh_s.at[c, 0], vh_r.at[c, 0], st=xm),
             remote(six(vs[c], 42), six(vs[c], 30), vh_s.at[c, 1], vh_r.at[c, 1], st=xp)]
            for c in range(2)]

    def v_start(c):
        vleft[c][0].start()
        vright[c][1].start()
        vleft[c][1].start()
        vright[c][0].start()

    def v_hop(c):
        vleft[c][0].wait_recv()
        vhop[c][0].start()
        vright[c][1].wait_recv()
        vhop[c][1].start()

    def v_wait(c):
        vleft[c][1].wait_recv()
        vright[c][0].wait_recv()
        vhop[c][0].wait_recv()
        vhop[c][1].wait_recv()

    def rows(ref, s, half):
        return ref if s < 3 else ref.at[pl.ds(256 * half, 256), :]

    up, down, id_steps = [], [], []
    for s in range(4):
        a, b = (8 - s) % 8, 7 - s
        up.append(remote(rows(qq.at[a], s, 0), rows(qq.at[b], s, 0), zs.at[0, s], zr.at[0, s], st=zp))
        down.append(remote(rows(qq.at[s], s, 1), rows(qq.at[s + 1], s, 1), zs.at[1, s], zr.at[1, s], st=zm))
        steps = [remote(idv.at[a], idv.at[b], ids_s.at[0, s], ids_r.at[0, s], st=zp)]
        if s < 3:
            steps.append(remote(idv.at[s], idv.at[s + 1], ids_s.at[1, s], ids_r.at[1, s], st=zm))
        id_steps.append(steps)

    def z_start(s):
        up[s].start()
        down[s].start()

    def z_wait(s):
        up[s].wait_recv()
        down[s].wait_recv()

    def ids_start(s):
        for c in id_steps[s]:
            c.start()

    def ids_wait(s):
        for c in id_steps[s]:
            c.wait_recv()

    idv[0] = jnp.zeros((8, 128), jnp.int32)
    idv[0, 0:4, 0:8] = ids[...]
    loads["tok"].wait()
    loads["wq"].wait()
    proj = dg(tokv[...], wqv[...], 1, 0)
    qq[0] = (head_normed(proj) * qgain[...]).astype(BF) * BF(0.0625)
    ready()
    ids_start(0)
    z_start(0)
    loads["wk"].wait()
    loads["wv"].wait()
    for g in range(3):
        for i in ORDER[4 * g:4 * g + 4]:
            loads[i].wait()
        r = sv[4 * g:4 * g + 4].reshape(384, sv.shape[2])
        k = head_normed(dg(r, wkv[...], 1, 0)).astype(BF)
        for u, i in enumerate(ORDER[4 * g:4 * g + 4]):
            ks[i] = k[96 * u:96 * u + 96]
        left[g].start()
        right[g].start()
    left[3].start()
    right[3].start()
    ids_wait(0)
    ids_start(1)
    for g in range(3):
        v = dg(sv[4 * g:4 * g + 4].reshape(384, sv.shape[2]), wvv[...], 1, 0).astype(BF)
        for u, i in enumerate(ORDER[4 * g:4 * g + 4]):
            vs0[i] = v[96 * u:96 * u + 96, 0:128]
            vs1[i] = v[96 * u:96 * u + 96, 128:256]
    ids_wait(1)
    ids_start(2)
    for name in ("wg", "mq", "mk", "mv"):
        loads[name].wait()
    glow[...] = dg(tokv[...], wgv[...], 1, 0).astype(BF)
    stages = mixer_stages(tokv, mqv, mkv, mvv, wdl, wdu, base, shift, wrl, wru, gain, heads,
                          s_a, s_q, s_ki, s_ri, s_kf, s_rf, s_vs, s_e, s_o)
    next(stages)
    ids_wait(2)
    ids_start(3)
    z_wait(0)
    z_start(1)
    next(stages)
    for i in range(3):
        left[i].wait_recv()
    khop[0].start()
    for i in range(3):
        right[i].wait_recv()
    khop[1].start()
    v_start(0)
    next(stages)
    ids_wait(3)
    lstv[...] = slot_list(idv[...], z, x)
    put = pltpu.make_async_copy(lstv, lst, in_sem.at[len(loads)])
    put.start()
    next(stages)
    z_wait(1)
    z_start(2)
    for _ in stages:
        pass
    hspread = Spread(heads, head_all, sp_s.at[0], sp_r.at[0], yp, ym, sib)
    hspread.first(0)
    hspread.first(1)
    loads["wgu"].wait()
    loads["wm"].wait()
    loads["wc"].wait()
    gate[...] = jax.nn.sigmoid(dg(glow[...], wguv[...], 1, 0))
    put.wait()

    lane = lax.broadcasted_iota(jnp.int32, (8, 768), 1)
    r128 = lax.broadcasted_iota(jnp.int32, (128, 768), 0)
    diag = lax.broadcasted_iota(jnp.int32, (64, 128), 0) == lax.broadcasted_iota(jnp.int32, (64, 128), 1)

    def slot(d, r):
        return jnp.minimum(jnp.maximum(lst[d, r], 0), 47)

    def scores(d, u):
        block = jnp.zeros((8, 768), jnp.int32)
        for r in range(8):
            kd[u, 96 * r:96 * r + 96, :] = ks[slot(d, r)]
            block = jnp.where((lane >= 96 * r) & (lane < 96 * r + 96), lst[d, 64 + r], block)
        block = block[0:1]
        sums = []
        for t in range(4):
            s = slice(128 * t, 128 * t + 128)
            p = jnp.exp(dg(qq[d, s, :], kd[u], 1, 1))
            p = jnp.where(r128 // 64 + (2 * t + 1) == block, p, 0.0)
            pbuf[d, s, :] = p.astype(BF)
            total = jnp.sum(p, axis=1, keepdims=True)
            for v in range(2):
                line = jnp.where(diag, total[64 * v:64 * v + 64], 0.0)
                sums.append(jnp.sum(line, axis=0, keepdims=True))
        den[8 * d:8 * d + 8, :] = jnp.concatenate(sums, axis=0)

    def values(c, d, u):
        for r in range(8):
            vd[u, 96 * r:96 * r + 96, :] = vs[c][slot(d, r)]
        part[c, d] = dg(pbuf[d], vd[u], 1, 0)

    hspread.second(0)
    hspread.second(1)
    left[3].wait_recv()
    right[3].wait_recv()
    khop[0].wait_recv()
    khop[1].wait_recv()
    for n, d in enumerate((0, 1, 7)):
        scores(d, n % 2)
    z_wait(2)
    z_start(3)
    scores(2, 1)
    v_hop(0)
    v_start(1)
    scores(6, 0)
    scores(3, 1)
    scores(5, 0)
    origin = [[lax.rem(y + r, 4) * 2 + (core if c == 0 else 1 - core) for r in range(4)] for c in range(2)]
    rest = [(c, r) for c in range(2) for r in range(4) if (c, r) != (0, 0)]

    def weight(w, size, c, r, shift_rows):
        at = pl.multiple_of(origin[c][r] * size + shift_rows, 128)
        return w[pl.ds(at, 128), :]

    hspread.third(0)
    hspread.third(1)
    z_wait(3)
    scores(4, 1)
    for h in range(2):
        hspread.arrived(h, 0, 3, 4, 6)
        m = dg(heads[256 * h:256 * h + 256, :], weight(wmv, 128, 0, 0, 0), 1, 0)
        for c, r in rest:
            m = m + dg(head_all[c, r, h], weight(wmv, 128, c, r, 0), 1, 0)
        mixed[256 * h:256 * h + 256, :] = m

    to = {"st_up": zp, "st_down": zm}

    def box_rows(ref, c, p, s):
        return ref.at[c, p, s] if c == 0 else ref.at[c, p, s, pl.ds(0, 256), :]

    sends = [[[remote(box_rows(msg, c, p, s), box_rows(box, c, p, s), ps.at[c, p, s], pr.at[c, p, s], st=to[way])
               for s in range(len(ds))] for p, (way, _, ds) in enumerate(PIPES)] for c in range(2)]

    def own(c, d, h):
        return part[c, d, 256 * h:256 * h + 256, :], den[8 * d:8 * d + 8, 0:64]

    def held(c, p, s):
        n = box[c, p, s, 0:256, :].astype(F32)
        if c == 1:
            return n, 0.0
        line = box[c, p, s, 256:272, :].astype(F32)[0:8]
        return n, line[:, 0:64] + line[:, 64:128]

    def send(c, p, s):
        _, h, ds = PIPES[p]
        n, d = own(c, ds[s], h)
        if s:
            sends[c][p][s - 1].wait_recv()
            n2, d2 = held(c, p, s - 1)
            n, d = n + n2, d + d2
        msg[c, p, s, 0:256, :] = n.astype(BF)
        if c == 0:
            hi = d.astype(BF).astype(F32)
            line = jnp.concatenate([hi, d - hi], axis=1)
            msg[c, p, s, 256:272, :] = jnp.concatenate([line, jnp.zeros((8, 128), F32)], axis=0).astype(BF)
        sends[c][p][s].start()

    inverse = [None, None]
    spread = [Spread(att.at[c], att_all.at[c], sp_s.at[1 + c], sp_r.at[1 + c], yp, ym, sib) for c in range(2)]

    def settle(c):
        for h, pipes in ((0, (3, 0)), (1, (2, 1))):
            n, d = own(c, 0, h)
            for p in pipes:
                s = len(PIPES[p][2]) - 1
                sends[c][p][s].wait_recv()
                n2, d2 = held(c, p, s)
                n, d = n + n2, d + d2
            if c == 0:
                inverse[h] = jnp.transpose(1.0 / d)
            for b in range(4):
                col = 4 * h + b
                att[c, 256 * h + 64 * b:256 * h + 64 * b + 64, :] = (
                    n[64 * b:64 * b + 64] * inverse[h][:, col:col + 1]).astype(BF)
            spread[c].first(h)

    def begin(c):
        values(c, 4, 0)
        send(c, 0, 0)
        send(c, 1, 0)
        values(c, 3, 1)
        send(c, 2, 0)
        values(c, 5, 0)
        send(c, 3, 0)
        for n, d in enumerate((2, 6, 1, 7, 0)):
            values(c, d, (n + 1) % 2)

    def step(c, s):
        for p in range(4):
            if s < len(PIPES[p][2]):
                send(c, p, s)

    def add(acc, c, h, which):
        for q, r in which:
            acc = acc + dg(att_all[c, q, r, h], weight(wcv, 256, q, r, 128 * c), 1, 0)
        return acc

    v_wait(0)
    begin(0)
    v_hop(1)
    step(0, 1)
    step(0, 2)
    v_wait(1)
    begin(1)
    step(0, 3)
    step(1, 1)
    settle(0)
    step(1, 2)
    spread[0].second(0)
    spread[0].second(1)
    step(1, 3)
    spread[0].third(0)
    spread[0].third(1)
    acc = []
    for h in range(2):
        a = dg(att[0, 256 * h:256 * h + 256, :], weight(wcv, 256, 0, 0, 0), 1, 0)
        spread[0].arrived(h, 0, 3, 4, 6)
        acc.append(add(a, 0, h, rest))
    settle(1)
    for h in range(2):
        acc[h] = acc[h] + dg(att[1, 256 * h:256 * h + 256, :], weight(wcv, 256, 0, 0, 128), 1, 0)
    spread[1].second(0)
    spread[1].second(1)
    for h in range(2):
        spread[1].arrived(h, 0)
        acc[h] = add(acc[h], 1, h, ((0, 3), (0, 1), (1, 0)))
    spread[1].third(0)
    spread[1].third(1)
    for h in range(2):
        spread[1].arrived(h, 3, 4)
        acc[h] = add(acc[h], 1, h, ((0, 2), (1, 1), (1, 3)))
    for h in range(2):
        spread[1].arrived(h, 6)
        c = add(acc[h], 1, h, ((1, 2),))
        s = slice(256 * h, 256 * h + 256)
        out[s, :] = (mixed[s, :] + gate[s, :] * c).astype(BF)
    for group in (left, right, khop, *vleft, *vright, *vhop, up, down, *id_steps,
                  *sends[0], *sends[1], *(p for sp in (hspread, *spread) for p in sp.copies)):
        for c in group:
            c.wait_send()


def local(
    tokens, mix_query, mix_key, mix_value, decay_lower_map, decay_upper_map, decay_base,
    decay_shift, rate_lower_map, rate_upper_map, norm_gain, mix_out, cross_query, score_gain,
    passage_key, passage_value, cross_out, gate_down, gate_up, store, passage_ids,
):
    rows, width = tokens.shape
    sds = jax.ShapeDtypeStruct
    vm = pltpu.VMEM
    dma = pltpu.SemaphoreType.DMA
    f = lambda: vm((rows, 128), F32)
    b = lambda: vm((rows, 128), BF)
    w256 = lambda: vm((width, 256), BF)
    w128 = lambda: vm((width, 128), BF)
    return pl.pallas_call(
        layer_kernel,
        out_shape=sds((rows, 256), BF),
        in_specs=[ANY] * 12 + [VMEM] * 9,
        out_specs=VMEM,
        scratch_shapes=[
            vm((12, 96, width), BF), w256(), w256(), vm((rows, width), BF), w256(), w128(), w128(),
            w128(), w128(), vm(cross_out.shape, BF), vm(mix_out.shape, BF), vm(gate_up.shape, BF),
            vm((48, 96, 256), BF), vm((48, 96, 128), BF), vm((48, 96, 128), BF), vm((NZ, rows, 256), BF),
            vm((8, 8, 128), jnp.int32), vm((8, 128), jnp.int32), pltpu.SMEM((8, 128), jnp.int32), b(), b(),
            f(), f(), b(), b(), b(), b(), b(), vm((8, 128), F32), f(),
            vm((2, 768, 256), BF), vm((2, 768, 128), BF), vm((NZ, rows, 768), BF),
            vm((2, NZ, rows, 128), F32), vm((64, 128), F32),
            vm((2, 4, 4, 272, 128), BF), vm((2, 4, 4, 272, 128), BF), vm((2, 4, 2, 256, 128), BF),
            vm((2, rows, 128), BF), vm((2, 2, 4, 2, 256, 128), BF), vm((rows, 256), F32), vm((rows, 256), F32),
            dma((24,)), dma((2, 4)), dma((2, 4)), dma((2,)), dma((2,)), dma((2, 2, 2)), dma((2, 2, 2)),
            dma((2, 2)), dma((2, 2)), dma((2, 4)), dma((2, 4)), dma((2, 4)), dma((2, 4)),
            dma((2, 4, 4)), dma((2, 4, 4)), dma((3, 2, 7)), dma((3, 2, 7)),
        ],
        compiler_params=params(62, collective_id=0, has_side_effects=True),
        cost_estimate=cost(3e10),
        name="layer",
    )(store, passage_key, passage_value, tokens, cross_query, gate_down, mix_query, mix_key, mix_value,
      cross_out, mix_out, gate_up, score_gain[None], passage_ids.T, decay_lower_map.T, decay_upper_map,
      decay_base[None], decay_shift.T, rate_lower_map.T, rate_upper_map, norm_gain[None])


def solution(mesh):
    placed = (
        P("st", None), P(None, "tp"), P(None, "tp"), P(None, "tp"), P(), P(None, "tp"), P("tp"),
        P("st", "tp"), P(), P(None, "tp"), P("tp"), P(None, "tp"), P(None, "tp"), P("tp"),
        P(None, "tp"), P(None, "tp"), P(None, "tp"), P(), P(None, "tp"), P("st", None, None),
        P("st", None),
    )
    return jax.shard_map(
        local, mesh=mesh, in_specs=placed, out_specs=P("st", "tp"), check_vma=False)
```

```python
import functools
import math

import jax
import jax.numpy as jnp
from jax import lax
from jax.experimental import pallas as pl
from jax.experimental.pallas import tpu as pltpu
from jax.sharding import PartitionSpec as P

F32 = jnp.float32
BF = jnp.bfloat16
NZ, NX = 8, 4
QBLOCK = 64
VMEM = pl.BlockSpec(memory_space=pltpu.VMEM)
MESH = pl.DeviceIdType.MESH
HBM = pl.BlockSpec(memory_space=pltpu.HBM)
SMEM = pl.BlockSpec(memory_space=pltpu.SMEM)
ANY = pl.BlockSpec(memory_space=pl.ANY)


def dg(a, b, ca, cb):
    return lax.dot_general(a, b, (((ca,), (cb,)), ((), ())), preferred_element_type=F32)


def bdot(a, b, ca=1, cb=0):
    return dg(a.astype(BF), b.astype(BF), ca, cb)


def cost(flops):
    return pl.CostEstimate(flops=int(flops), bytes_accessed=int(4e6), transcendentals=0)


def params(mib, **kw):
    return pltpu.CompilerParams(vmem_limit_bytes=mib * 1024 * 1024, **kw)


def head_normed(y):
    return y * lax.rsqrt(jnp.mean(y * y, axis=-1, keepdims=True) + 1e-06)


def exact_sum_dot(left, x, ca, cb, swap):
    hi = x.astype(BF)
    r = x - hi.astype(F32)
    mid = r.astype(BF)
    low = (r - mid.astype(F32)).astype(BF)
    parts = [dg(p, left, ca, cb) if swap else dg(left, p, ca, cb) for p in (hi, mid, low)]
    return parts[0] + parts[1] + parts[2]


def mixer_stages(tok, wq, wk, wv, wdl, wdu, base, shift, wrl, wru, gain, out,
                 s_a, s_q, s_ki, s_ri, s_kf, s_rf, s_vs, s_e, s_o):
    t = tok[...]
    rows = t.shape[0]
    chunks = rows // 64
    lane = lax.broadcasted_iota(jnp.int32, (64, 128), 1)
    row = lax.broadcasted_iota(jnp.int32, (64, 128), 0)
    left = lane < 64
    in_head = jnp.where(left, lane, lane - 64)
    sl = left & (in_head < row)
    sr = jnp.logical_not(left) & (in_head < row)
    upto = in_head <= row
    r2 = lax.broadcasted_iota(jnp.int32, (128, 128), 0)
    l2 = lax.broadcasted_iota(jnp.int32, (128, 128), 1)
    same = (r2 < 64) == (l2 < 64)
    eye = r2 == l2
    ones = jnp.where(same, 1.0, 0.0).astype(BF)
    tri = jnp.where(
        lax.broadcasted_iota(jnp.int32, (64, 64), 1) <= lax.broadcasted_iota(jnp.int32, (64, 64), 0),
        1.0, 0.0).astype(BF)
    q = dg(t, wq[...], 1, 0).astype(BF).astype(F32)
    k = dg(t, wk[...], 1, 0).astype(BF).astype(F32)
    v = dg(t, wv[...], 1, 0).astype(BF).astype(F32)
    low = jnp.tanh(dg(t, wdl[...], 1, 1)).astype(BF)
    spread2 = jnp.where(
        (lax.broadcasted_iota(jnp.int32, (2, 128), 1) < 64)
        == (lax.broadcasted_iota(jnp.int32, (2, 128), 0) == 0), 1.0, 0.0).astype(BF)
    pre = base[...] + dg(low, wdu[...], 1, 0) + exact_sum_dot(spread2, shift[...], 0, 0, True)
    log_fade = jax.nn.sigmoid(pre) * (-math.exp(-0.5))
    rate_low = dg(t, wrl[...], 1, 1).astype(BF)
    rate = jax.nn.sigmoid(dg(rate_low, wru[...], 1, 0))
    yield
    unit = k * lax.rsqrt(exact_sum_dot(ones, k * k, 1, 0, True) + 1e-06)
    rate_key = unit * rate
    s_vs[...] = pltpu.roll(v, 64, 1).astype(BF)
    for c in range(chunks):
        s = slice(64 * c, 64 * c + 64)
        f = log_fade[s]
        cumul = exact_sum_dot(tri, f, 1, 0, False)
        end = cumul[63:64]
        ei = jnp.exp(-cumul)
        fo = jnp.exp(end - cumul)
        s_a[s, :] = -unit[s] * jnp.exp(cumul - f)
        s_q[s, :] = q[s] * jnp.exp(cumul)
        s_ki[s, :] = (k[s] * ei).astype(BF)
        s_ri[s, :] = (rate_key[s] * ei).astype(BF)
        s_kf[s, :] = (k[s] * fo).astype(BF)
        s_rf[s, :] = (rate_key[s] * fo).astype(BF)
        s_e[c:c + 1, :] = jnp.exp(end)

    yield
    zb = jnp.zeros((64, 128), BF)
    zf = jnp.zeros((64, 128), F32)

    def only(x, m):
        return jnp.where(m, x, zb if x.dtype == BF else zf)

    right = jnp.logical_not(left)
    cat = jnp.concatenate
    group = 4
    state = jnp.zeros((128, 128), F32)
    for g in range(chunks // group):
        cs = [slice(64 * c, 64 * c + 64) for c in range(g * group, (g + 1) * group)]
        G0, G1, PW, X, VL, VR = [], [], [], [], [], []
        for s in cs:
            a, qq = s_a[s, :].astype(BF), s_q[s, :].astype(BF)
            ki, ri = s_ki[s, :], s_ri[s, :]
            G0.append(dg(cat([only(a, left), only(qq, left)], 0), cat([ri, ki], 0), 1, 1))
            G1.append(dg(cat([only(a, right), only(qq, right)], 0), cat([ki, ri], 0), 1, 1))
        for i, s in enumerate(cs):
            vs = s_vs[s, :]
            VR.append(only(vs, right))
            VL.append(only(vs, left))
            L = cat([only(G0[i][:64], sr), only(G1[i][:64], sl)], 0)
            PW.append(cat([only(G0[i][:64], sl), only(G1[i][:64], sr)], 0))
            a = s_a[s, :]
            X.append(cat([only(a, left), only(a, right)], 0) + bdot(L, cat([VL[i], VR[i]], 0)))
        for it in range(6):
            for i in range(group):
                p16 = PW[i].astype(BF)
                if it < 5:
                    px = dg(p16, cat([p16, X[i].astype(BF)], 1), 1, 0)
                    PW[i] = px[:, :128]
                    X[i] = X[i] + px[:, 128:]
                else:
                    X[i] = X[i] + dg(p16, X[i].astype(BF), 1, 0)
        MM, NN, PC, OO = [], [], [], []
        for i, s in enumerate(cs):
            x16 = X[i].astype(BF)
            h0 = cat([x16[:64], VR[i]], 0)
            h1 = cat([VL[i], x16[64:]], 0)
            y0 = bdot(only(G0[i][64:], upto), h0)
            y1 = bdot(only(G1[i][64:], upto), h1)
            qq = s_q[s, :]
            PC.append(cat([only(y0 + qq, left), only(y1 + qq, right)], 0).astype(BF))
            OO.append(only(y0, right) + only(y1, left))
            kf, rf = s_kf[s, :], s_rf[s, :]
            f = cat([only(rf, left), only(kf, left), only(kf, right), only(rf, right)], 0)
            tr = dg(cat([h0, h1], 0), f, 0, 0)
            e = s_e[g * group + i:g * group + i + 1, :]
            zz = jnp.zeros((128, 128), F32)
            MM.append((jnp.where(same, tr, zz) + jnp.where(eye, e, zz)).astype(BF))
            NN.append(jnp.where(same, zz, tr))
        for i, s in enumerate(cs):
            s16 = state.astype(BF)
            o = dg(PC[i], s16, 1, 1)
            s_o[s, :] = OO[i] + o[:64] + o[64:]
            state = dg(s16, MM[i], 1, 0) + NN[i]
        yield
    o = pltpu.roll(s_o[...], 64, 1)
    centred = o - exact_sum_dot(ones, o, 1, 0, True) * (1.0 / 64)
    spread = exact_sum_dot(ones, centred * centred, 1, 0, True) * (1.0 / 64)
    out[...] = (centred * lax.rsqrt(spread + 0.00064) * gain[...]).astype(BF)


ORDER = (0, 1, 6, 7, 2, 3, 8, 9, 4, 5, 10, 11)


def remote(src, dst, send, recv, **device):
    return pltpu.make_async_remote_copy(
        src_ref=src, dst_ref=dst, send_sem=send, recv_sem=recv, device_id=device,
        device_id_type=MESH)


def meet(peers):
    barrier = pltpu.get_barrier_semaphore()
    for device in peers:
        pl.semaphore_signal(barrier, inc=1, device_id=device, device_id_type=MESH)
    return lambda: pl.semaphore_wait(barrier, len(peers))


def slot_list(ids, z, x):
    row = lax.broadcasted_iota(jnp.int32, (64, 128), 0)
    lane = lax.broadcasted_iota(jnp.int32, (64, 128), 1)
    valid = (row - 8 * (row // 8) < 4) & (lane < 8)
    p = ids.reshape(64, 128).astype(F32)
    plane = jnp.floor((p + 0.5) * (1.0 / 48))
    owner = jnp.floor((p + 0.5) * (1.0 / 12))
    step = owner - 4 * plane - x.astype(F32)
    step = jnp.where(step < 0, step + 4, step)
    slot = step * 12 + p - 12 * owner
    hit = valid & (plane == z.astype(F32))
    m = jnp.where(hit, 1.0, 0.0)
    r1 = lax.broadcasted_iota(jnp.int32, (64, 64), 0)
    c1 = lax.broadcasted_iota(jnp.int32, (64, 64), 1)
    r2 = lax.broadcasted_iota(jnp.int32, (128, 128), 0)
    c2 = lax.broadcasted_iota(jnp.int32, (128, 128), 1)
    near = r1 // 8 == c1 // 8
    above = bdot(jnp.where(near & (c1 < r1), 1.0, 0.0), m)
    column = bdot(jnp.where(near, 1.0, 0.0), m)
    pos = above + bdot(column, jnp.where(r2 < c2, 1.0, 0.0))
    pos = jnp.where(hit, pos, -1.0)
    lanes = lane.astype(F32)
    acc = jnp.zeros((64, 128), F32)
    for b in range(8):
        at = pos[:, b:b + 1]
        acc = acc + jnp.where(at == lanes, slot[:, b:b + 1], 0.0)
        acc = acc + jnp.where((at == lanes - 64) & (at >= 0), b + 1.0, 0.0)
    return jnp.sum(acc.reshape(8, 8, 128), axis=1).astype(jnp.int32)


PIPES = (("st_up", 0, (4, 3, 2, 1)), ("st_down", 1, (4, 5, 6, 7)),
         ("st_up", 1, (3, 2, 1)), ("st_down", 0, (5, 6, 7)))


class Spread:
    def __init__(self, own, buf, send, recv, yp, ym, sib):
        self.copies = []
        for h in range(2):
            s = own.at[pl.ds(256 * h, 256), :]
            links = [(s, buf.at[1, 0, h], sib), (s, buf.at[0, 3, h], yp), (s, buf.at[0, 1, h], ym),
                     (buf.at[0, 3, h], buf.at[1, 3, h], sib), (buf.at[0, 1, h], buf.at[1, 1, h], sib),
                     (buf.at[0, 3, h], buf.at[0, 2, h], yp) if h == 0
                     else (buf.at[0, 1, h], buf.at[0, 2, h], ym),
                     (buf.at[0, 2, h], buf.at[1, 2, h], sib)]
            self.copies.append([
                remote(a, b, send.at[h, k], recv.at[h, k], tp=to) for k, (a, b, to) in enumerate(links)])

    def first(self, h):
        c = self.copies[h]
        for k in ((1, 2, 0) if h == 0 else (2, 1, 0)):
            c[k].start()

    def second(self, h):
        c = self.copies[h]
        if h == 0:
            c[1].wait_recv()
            c[5].start()
            c[3].start()
            c[2].wait_recv()
            c[4].start()
        else:
            c[2].wait_recv()
            c[5].start()
            c[4].start()
            c[1].wait_recv()
            c[3].start()

    def third(self, h):
        self.copies[h][5].wait_recv()
        self.copies[h][6].start()

    def arrived(self, h, *which):
        for k in which:
            self.copies[h][k].wait_recv()


def layer_kernel(store, wk, wv, tok, wq, wg, mq, mk, mv, wc, wm, wgu, qgain, ids, wdl, wdu, base, shift, wrl,
                 wru, gain, out,
                 sv, wkv, wvv, tokv, wqv, wgv, mqv, mkv, mvv, wcv, wmv, wguv, ks, vs0, vs1, qq, idv, lstv, lst,
                 glow, heads, s_a, s_q, s_ki, s_ri, s_kf, s_rf, s_vs, s_e, s_o,
                 kd, vd, pbuf, part, den, msg, box, head_all, att, att_all, gate, mixed,
                 in_sem, k_s, k_r, kh_s, kh_r, v_s, v_r, vh_s, vh_r, zs, zr, ids_s, ids_r, ps, pr, sp_s, sp_r):
    vs = (vs0, vs1)
    st, tp = lax.axis_index("st"), lax.axis_index("tp")
    z, x = st // NX, lax.rem(st, NX)
    y, core = tp // 2, lax.rem(tp, 2)
    xp = z * NX + lax.rem(x + 1, NX)
    xm = z * NX + lax.rem(x + NX - 1, NX)
    zp = lax.rem(z + 1, NZ) * NX + x
    zm = lax.rem(z + NZ - 1, NZ) * NX + x
    yp = lax.rem(y + 1, 4) * 2 + core
    ym = lax.rem(y + 3, 4) * 2 + core
    sib = y * 2 + 1 - core
    ready = meet([{"st": xp}, {"st": xm}, {"st": zp}, {"st": zm}, {"tp": yp}, {"tp": ym}, {"tp": sib}])
    loads = {}

    def load(name, src, dst):
        loads[name] = pltpu.make_async_copy(src, dst, in_sem.at[len(loads)])
        loads[name].start()

    load("tok", tok, tokv)
    load("wq", wq, wqv)
    load("wk", wk, wkv)
    load("wv", wv, wvv)
    for p, i in enumerate(ORDER):
        load(i, store.at[i], sv.at[p])
    for name, src, dst in (("wg", wg, wgv), ("mq", mq, mqv), ("mk", mk, mkv), ("mv", mv, mvv),
                           ("wm", wm, wmv), ("wgu", wgu, wguv), ("wc", wc, wcv)):
        load(name, src, dst)

    def six(ref, at, n=6):
        return ref.at[pl.ds(at, n)]

    left = [remote(six(ks, a, n), six(ks, 12 + a, n), k_s.at[0, i], k_r.at[0, i], st=xm)
            for i, (a, n) in enumerate(((0, 2), (2, 2), (4, 2), (6, 6)))]
    right = [remote(six(ks, a, n), six(ks, 36 + a, n), k_s.at[1, i], k_r.at[1, i], st=xp)
             for i, (a, n) in enumerate(((6, 2), (8, 2), (10, 2), (0, 6)))]

    khop = [remote(six(ks, 12), six(ks, 24), kh_s.at[0], kh_r.at[0], st=xm),
            remote(six(ks, 42), six(ks, 30), kh_s.at[1], kh_r.at[1], st=xp)]
    vleft = [[remote(six(vs[c], 6 * i), six(vs[c], 12 + 6 * i), v_s.at[c, 0, i], v_r.at[c, 0, i], st=xm)
              for i in range(2)] for c in range(2)]
    vright = [[remote(six(vs[c], 6 * i), six(vs[c], 36 + 6 * i), v_s.at[c, 1, i], v_r.at[c, 1, i], st=xp)
               for i in range(2)] for c in range(2)]
    vhop = [[remote(six(vs[c], 12), six(vs[c], 24), vh_s.at[c, 0], vh_r.at[c, 0], st=xm),
             remote(six(vs[c], 42), six(vs[c], 30), vh_s.at[c, 1], vh_r.at[c, 1], st=xp)]
            for c in range(2)]

    def v_start(c):
        vleft[c][0].start()
        vright[c][1].start()
        vleft[c][1].start()
        vright[c][0].start()

    def v_hop(c):
        vleft[c][0].wait_recv()
        vhop[c][0].start()
        vright[c][1].wait_recv()
        vhop[c][1].start()

    def v_wait(c):
        vleft[c][1].wait_recv()
        vright[c][0].wait_recv()
        vhop[c][0].wait_recv()
        vhop[c][1].wait_recv()

    pieces, id_steps = {}, []
    for s in range(4):
        a, b = (8 - s) % 8, 7 - s
        for h in range(2):
            at = pl.ds(256 * h, 256)
            both = []
            if s < 3 or h == 0:
                both.append(remote(qq.at[a, at, :], qq.at[b, at, :], zs.at[0, s, h], zr.at[0, s, h], st=zp))
            if s < 3 or h == 1:
                both.append(remote(qq.at[s, at, :], qq.at[s + 1, at, :], zs.at[1, s, h], zr.at[1, s, h], st=zm))
            pieces[s, h] = both
        steps = [remote(idv.at[a], idv.at[b], ids_s.at[0, s], ids_r.at[0, s], st=zp)]
        if s < 3:
            steps.append(remote(idv.at[s], idv.at[s + 1], ids_s.at[1, s], ids_r.at[1, s], st=zm))
        id_steps.append(steps)

    def z_start(s, h):
        for c in pieces[s, h]:
            c.start()

    def z_wait(s, h):
        for c in pieces[s, h]:
            c.wait_recv()

    def z_pass(s, h):
        z_wait(s, h)
        z_start(s + 1, h)

    def ids_start(s):
        for c in id_steps[s]:
            c.start()

    def ids_wait(s):
        for c in id_steps[s]:
            c.wait_recv()

    idv[0] = jnp.zeros((8, 128), jnp.int32)
    idv[0, 0:4, 0:8] = ids[...]
    loads["tok"].wait()
    loads["wq"].wait()
    proj = dg(tokv[...], wqv[...], 1, 0)
    qq[0] = (head_normed(proj) * qgain[...]).astype(BF) * BF(0.0625)
    ready()
    ids_start(0)
    z_start(0, 0)
    z_start(0, 1)
    loads["wk"].wait()
    loads["wv"].wait()
    for g in range(3):
        for i in ORDER[4 * g:4 * g + 4]:
            loads[i].wait()
        r = sv[4 * g:4 * g + 4].reshape(384, sv.shape[2])
        k = head_normed(dg(r, wkv[...], 1, 0)).astype(BF)
        for u, i in enumerate(ORDER[4 * g:4 * g + 4]):
            ks[i] = k[96 * u:96 * u + 96]
        left[g].start()
        right[g].start()
    left[3].start()
    right[3].start()
    ids_wait(0)
    ids_start(1)
    for g in range(3):
        v = dg(sv[4 * g:4 * g + 4].reshape(384, sv.shape[2]), wvv[...], 1, 0).astype(BF)
        for u, i in enumerate(ORDER[4 * g:4 * g + 4]):
            vs0[i] = v[96 * u:96 * u + 96, 0:128]
            vs1[i] = v[96 * u:96 * u + 96, 128:256]
    ids_wait(1)
    ids_start(2)
    for name in ("wg", "mq", "mk", "mv"):
        loads[name].wait()
    glow[...] = dg(tokv[...], wgv[...], 1, 0).astype(BF)
    stages = mixer_stages(tokv, mqv, mkv, mvv, wdl, wdu, base, shift, wrl, wru, gain, heads,
                          s_a, s_q, s_ki, s_ri, s_kf, s_rf, s_vs, s_e, s_o)
    ids_wait(2)
    ids_start(3)
    z_pass(0, 0)
    next(stages)
    z_pass(0, 1)
    next(stages)
    ids_wait(3)
    lstv[...] = slot_list(idv[...], z, x)
    put = pltpu.make_async_copy(lstv, lst, in_sem.at[len(loads)])
    put.start()
    for i in range(3):
        left[i].wait_recv()
    khop[0].start()
    for i in range(3):
        right[i].wait_recv()
    khop[1].start()
    v_start(0)
    z_pass(1, 0)
    next(stages)
    z_pass(1, 1)
    next(stages)
    z_pass(2, 0)
    for _ in stages:
        pass
    hspread = Spread(heads, head_all, sp_s.at[0], sp_r.at[0], yp, ym, sib)
    hspread.first(0)
    hspread.first(1)
    loads["wgu"].wait()
    loads["wm"].wait()
    loads["wc"].wait()
    gate[...] = jax.nn.sigmoid(dg(glow[...], wguv[...], 1, 0))
    put.wait()
    z_pass(2, 1)

    lane = lax.broadcasted_iota(jnp.int32, (8, 768), 1)
    r128 = lax.broadcasted_iota(jnp.int32, (128, 768), 0)
    diag = lax.broadcasted_iota(jnp.int32, (64, 128), 0) == lax.broadcasted_iota(jnp.int32, (64, 128), 1)

    def slot(d, r):
        return jnp.minimum(jnp.maximum(lst[d, r], 0), 47)

    def scores(d, u):
        block = jnp.zeros((8, 768), jnp.int32)
        for r in range(8):
            kd[u, 96 * r:96 * r + 96, :] = ks[slot(d, r)]
            block = jnp.where((lane >= 96 * r) & (lane < 96 * r + 96), lst[d, 64 + r], block)
        block = block[0:1]
        sums = []
        for t in range(4):
            s = slice(128 * t, 128 * t + 128)
            p = jnp.exp(dg(qq[d, s, :], kd[u], 1, 1))
            p = jnp.where(r128 // 64 + (2 * t + 1) == block, p, 0.0)
            pbuf[d, s, :] = p.astype(BF)
            total = jnp.sum(p, axis=1, keepdims=True)
            for v in range(2):
                line = jnp.where(diag, total[64 * v:64 * v + 64], 0.0)
                sums.append(jnp.sum(line, axis=0, keepdims=True))
        den[8 * d:8 * d + 8, :] = jnp.concatenate(sums, axis=0)

    def values(c, d, u):
        for r in range(8):
            vd[u, 96 * r:96 * r + 96, :] = vs[c][slot(d, r)]
        part[c, d] = dg(pbuf[d], vd[u], 1, 0)

    hspread.second(0)
    hspread.second(1)
    left[3].wait_recv()
    right[3].wait_recv()
    khop[0].wait_recv()
    khop[1].wait_recv()
    for n, d in enumerate((0, 1, 7)):
        scores(d, n % 2)
    scores(2, 1)
    scores(6, 0)
    v_hop(0)
    v_start(1)
    scores(3, 1)
    scores(5, 0)
    origin = [[lax.rem(y + r, 4) * 2 + (core if c == 0 else 1 - core) for r in range(4)] for c in range(2)]
    rest = [(c, r) for c in range(2) for r in range(4) if (c, r) != (0, 0)]

    def weight(w, size, c, r, shift_rows):
        at = pl.multiple_of(origin[c][r] * size + shift_rows, 128)
        return w[pl.ds(at, 128), :]

    hspread.third(0)
    hspread.third(1)
    z_wait(3, 0)
    z_wait(3, 1)
    scores(4, 1)
    for h in range(2):
        hspread.arrived(h, 0, 3, 4, 6)
        m = dg(heads[256 * h:256 * h + 256, :], weight(wmv, 128, 0, 0, 0), 1, 0)
        for c, r in rest:
            m = m + dg(head_all[c, r, h], weight(wmv, 128, c, r, 0), 1, 0)
        mixed[256 * h:256 * h + 256, :] = m

    to = {"st_up": zp, "st_down": zm}

    def box_rows(ref, c, p, s):
        return ref.at[c, p, s] if c == 0 else ref.at[c, p, s, pl.ds(0, 256), :]

    sends = [[[remote(box_rows(msg, c, p, s), box_rows(box, c, p, s), ps.at[c, p, s], pr.at[c, p, s], st=to[way])
               for s in range(len(ds))] for p, (way, _, ds) in enumerate(PIPES)] for c in range(2)]

    def own(c, d, h):
        return part[c, d, 256 * h:256 * h + 256, :], den[8 * d:8 * d + 8, 0:64]

    def held(c, p, s):
        n = box[c, p, s, 0:256, :].astype(F32)
        if c == 1:
            return n, 0.0
        line = box[c, p, s, 256:272, :].astype(F32)[0:8]
        return n, line[:, 0:64] + line[:, 64:128]

    def send(c, p, s):
        _, h, ds = PIPES[p]
        n, d = own(c, ds[s], h)
        if s:
            sends[c][p][s - 1].wait_recv()
            n2, d2 = held(c, p, s - 1)
            n, d = n + n2, d + d2
        msg[c, p, s, 0:256, :] = n.astype(BF)
        if c == 0:
            hi = d.astype(BF).astype(F32)
            line = jnp.concatenate([hi, d - hi], axis=1)
            msg[c, p, s, 256:272, :] = jnp.concatenate([line, jnp.zeros((8, 128), F32)], axis=0).astype(BF)
        sends[c][p][s].start()

    inverse = [None, None]
    spread = [Spread(att.at[c], att_all.at[c], sp_s.at[1 + c], sp_r.at[1 + c], yp, ym, sib) for c in range(2)]

    def settle(c):
        for h, pipes in ((0, (3, 0)), (1, (2, 1))):
            n, d = own(c, 0, h)
            for p in pipes:
                s = len(PIPES[p][2]) - 1
                sends[c][p][s].wait_recv()
                n2, d2 = held(c, p, s)
                n, d = n + n2, d + d2
            if c == 0:
                inverse[h] = jnp.transpose(1.0 / d)
            for b in range(4):
                col = 4 * h + b
                att[c, 256 * h + 64 * b:256 * h + 64 * b + 64, :] = (
                    n[64 * b:64 * b + 64] * inverse[h][:, col:col + 1]).astype(BF)
            spread[c].first(h)

    def begin(c):
        values(c, 4, 0)
        send(c, 0, 0)
        send(c, 1, 0)
        values(c, 3, 1)
        send(c, 2, 0)
        values(c, 5, 0)
        send(c, 3, 0)
        for n, d in enumerate((2, 6, 1, 7, 0)):
            values(c, d, (n + 1) % 2)

    def step(c, s):
        for p in range(4):
            if s < len(PIPES[p][2]):
                send(c, p, s)

    def add(acc, c, h, which):
        for q, r in which:
            acc = acc + dg(att_all[c, q, r, h], weight(wcv, 256, q, r, 128 * c), 1, 0)
        return acc

    v_wait(0)
    begin(0)
    v_hop(1)
    step(0, 1)
    step(0, 2)
    v_wait(1)
    begin(1)
    step(0, 3)
    step(1, 1)
    settle(0)
    step(1, 2)
    spread[0].second(0)
    spread[0].second(1)
    step(1, 3)
    spread[0].third(0)
    spread[0].third(1)
    acc = []
    for h in range(2):
        a = dg(att[0, 256 * h:256 * h + 256, :], weight(wcv, 256, 0, 0, 0), 1, 0)
        spread[0].arrived(h, 0, 3, 4, 6)
        acc.append(add(a, 0, h, rest))
    settle(1)
    for h in range(2):
        acc[h] = acc[h] + dg(att[1, 256 * h:256 * h + 256, :], weight(wcv, 256, 0, 0, 128), 1, 0)
    spread[1].second(0)
    spread[1].second(1)
    for h in range(2):
        spread[1].arrived(h, 0)
        acc[h] = add(acc[h], 1, h, ((0, 3), (0, 1), (1, 0)))
    spread[1].third(0)
    spread[1].third(1)
    for h in range(2):
        spread[1].arrived(h, 3, 4)
        acc[h] = add(acc[h], 1, h, ((0, 2), (1, 1), (1, 3)))
    for h in range(2):
        spread[1].arrived(h, 6)
        c = add(acc[h], 1, h, ((1, 2),))
        s = slice(256 * h, 256 * h + 256)
        out[s, :] = (mixed[s, :] + gate[s, :] * c).astype(BF)
    for group in (left, right, khop, *vleft, *vright, *vhop, *pieces.values(), *id_steps,
                  *sends[0], *sends[1], *(p for sp in (hspread, *spread) for p in sp.copies)):
        for c in group:
            c.wait_send()


def local(
    tokens, mix_query, mix_key, mix_value, decay_lower_map, decay_upper_map, decay_base,
    decay_shift, rate_lower_map, rate_upper_map, norm_gain, mix_out, cross_query, score_gain,
    passage_key, passage_value, cross_out, gate_down, gate_up, store, passage_ids,
):
    rows, width = tokens.shape
    sds = jax.ShapeDtypeStruct
    vm = pltpu.VMEM
    dma = pltpu.SemaphoreType.DMA
    f = lambda: vm((rows, 128), F32)
    b = lambda: vm((rows, 128), BF)
    w256 = lambda: vm((width, 256), BF)
    w128 = lambda: vm((width, 128), BF)
    return pl.pallas_call(
        layer_kernel,
        out_shape=sds((rows, 256), BF),
        in_specs=[ANY] * 12 + [VMEM] * 9,
        out_specs=VMEM,
        scratch_shapes=[
            vm((12, 96, width), BF), w256(), w256(), vm((rows, width), BF), w256(), w128(), w128(),
            w128(), w128(), vm(cross_out.shape, BF), vm(mix_out.shape, BF), vm(gate_up.shape, BF),
            vm((48, 96, 256), BF), vm((48, 96, 128), BF), vm((48, 96, 128), BF), vm((NZ, rows, 256), BF),
            vm((8, 8, 128), jnp.int32), vm((8, 128), jnp.int32), pltpu.SMEM((8, 128), jnp.int32), b(), b(),
            f(), f(), b(), b(), b(), b(), b(), vm((8, 128), F32), f(),
            vm((2, 768, 256), BF), vm((2, 768, 128), BF), vm((NZ, rows, 768), BF),
            vm((2, NZ, rows, 128), F32), vm((64, 128), F32),
            vm((2, 4, 4, 272, 128), BF), vm((2, 4, 4, 272, 128), BF), vm((2, 4, 2, 256, 128), BF),
            vm((2, rows, 128), BF), vm((2, 2, 4, 2, 256, 128), BF), vm((rows, 256), F32), vm((rows, 256), F32),
            dma((24,)), dma((2, 4)), dma((2, 4)), dma((2,)), dma((2,)), dma((2, 2, 2)), dma((2, 2, 2)),
            dma((2, 2)), dma((2, 2)), dma((2, 4, 2)), dma((2, 4, 2)), dma((2, 4)), dma((2, 4)),
            dma((2, 4, 4)), dma((2, 4, 4)), dma((3, 2, 7)), dma((3, 2, 7)),
        ],
        compiler_params=params(62, collective_id=0, has_side_effects=True),
        cost_estimate=cost(3e10),
        name="layer",
    )(store, passage_key, passage_value, tokens, cross_query, gate_down, mix_query, mix_key, mix_value,
      cross_out, mix_out, gate_up, score_gain[None], passage_ids.T, decay_lower_map.T, decay_upper_map,
      decay_base[None], decay_shift.T, rate_lower_map.T, rate_upper_map, norm_gain[None])


def solution(mesh):
    placed = (
        P("st", None), P(None, "tp"), P(None, "tp"), P(None, "tp"), P(), P(None, "tp"), P("tp"),
        P("st", "tp"), P(), P(None, "tp"), P("tp"), P(None, "tp"), P(None, "tp"), P("tp"),
        P(None, "tp"), P(None, "tp"), P(None, "tp"), P(), P(None, "tp"), P("st", None, None),
        P("st", None),
    )
    return jax.shard_map(
        local, mesh=mesh, in_specs=placed, out_specs=P("st", "tp"), check_vma=False)
```

```python
import functools
import math

import jax
import jax.numpy as jnp
from jax import lax
from jax.experimental import pallas as pl
from jax.experimental.pallas import tpu as pltpu
from jax.sharding import PartitionSpec as P

F32 = jnp.float32
BF = jnp.bfloat16
NZ, NX = 8, 4
QBLOCK = 64
VMEM = pl.BlockSpec(memory_space=pltpu.VMEM)
MESH = pl.DeviceIdType.MESH
HBM = pl.BlockSpec(memory_space=pltpu.HBM)
SMEM = pl.BlockSpec(memory_space=pltpu.SMEM)
ANY = pl.BlockSpec(memory_space=pl.ANY)


def dg(a, b, ca, cb):
    return lax.dot_general(a, b, (((ca,), (cb,)), ((), ())), preferred_element_type=F32)


def bdot(a, b, ca=1, cb=0):
    return dg(a.astype(BF), b.astype(BF), ca, cb)


def cost(flops):
    return pl.CostEstimate(flops=int(flops), bytes_accessed=int(4e6), transcendentals=0)


def params(mib, **kw):
    return pltpu.CompilerParams(vmem_limit_bytes=mib * 1024 * 1024, **kw)


def head_normed(y):
    return y * lax.rsqrt(jnp.mean(y * y, axis=-1, keepdims=True) + 1e-06)


def dg3(a, b, ca, cb):
    ah, bh = a.astype(BF), b.astype(BF)
    al, bl = (a - ah.astype(F32)).astype(BF), (b - bh.astype(F32)).astype(BF)
    return dg(ah, bh, ca, cb) + (dg(al, bh, ca, cb) + dg(ah, bl, ca, cb))


def exact_sum_dot(left, x, ca, cb, swap):
    hi = x.astype(BF)
    r = x - hi.astype(F32)
    mid = r.astype(BF)
    low = (r - mid.astype(F32)).astype(BF)
    parts = [dg(p, left, ca, cb) if swap else dg(left, p, ca, cb) for p in (hi, mid, low)]
    return parts[0] + parts[1] + parts[2]


def mixer_stages(tok, wq, wk, wv, wdl, wdu, base, shift, wrl, wru, gain, out,
                 s_a, s_q, s_ki, s_ri, s_kf, s_rf, s_vs, s_e, s_o):
    t = tok[...]
    rows = t.shape[0]
    chunks = rows // 64
    lane = lax.broadcasted_iota(jnp.int32, (64, 128), 1)
    row = lax.broadcasted_iota(jnp.int32, (64, 128), 0)
    left = lane < 64
    in_head = jnp.where(left, lane, lane - 64)
    sl = left & (in_head < row)
    sr = jnp.logical_not(left) & (in_head < row)
    upto = in_head <= row
    r2 = lax.broadcasted_iota(jnp.int32, (128, 128), 0)
    l2 = lax.broadcasted_iota(jnp.int32, (128, 128), 1)
    same = (r2 < 64) == (l2 < 64)
    eye = r2 == l2
    ones = jnp.where(same, 1.0, 0.0).astype(BF)
    tri = jnp.where(
        lax.broadcasted_iota(jnp.int32, (64, 64), 1) <= lax.broadcasted_iota(jnp.int32, (64, 64), 0),
        1.0, 0.0).astype(BF)
    q = dg(t, wq[...], 1, 0).astype(BF).astype(F32)
    k = dg(t, wk[...], 1, 0).astype(BF).astype(F32)
    v = dg(t, wv[...], 1, 0).astype(BF).astype(F32)
    low = jnp.tanh(dg(t, wdl[...], 1, 1)).astype(BF)
    spread2 = jnp.where(
        (lax.broadcasted_iota(jnp.int32, (2, 128), 1) < 64)
        == (lax.broadcasted_iota(jnp.int32, (2, 128), 0) == 0), 1.0, 0.0).astype(BF)
    pre = base[...] + dg(low, wdu[...], 1, 0) + exact_sum_dot(spread2, shift[...], 0, 0, True)
    log_fade = jax.nn.sigmoid(pre) * (-math.exp(-0.5))
    rate_low = dg(t, wrl[...], 1, 1).astype(BF)
    rate = jax.nn.sigmoid(dg(rate_low, wru[...], 1, 0))
    yield
    unit = k * lax.rsqrt(exact_sum_dot(ones, k * k, 1, 0, True) + 1e-06)
    rate_key = unit * rate
    s_vs[...] = pltpu.roll(v, 64, 1)
    for c in range(chunks):
        s = slice(64 * c, 64 * c + 64)
        f = log_fade[s]
        cumul = exact_sum_dot(tri, f, 1, 0, False)
        end = cumul[63:64]
        ei = jnp.exp(-cumul)
        fo = jnp.exp(end - cumul)
        s_a[s, :] = -unit[s] * jnp.exp(cumul - f)
        s_q[s, :] = q[s] * jnp.exp(cumul)
        s_ki[s, :] = k[s] * ei
        s_ri[s, :] = rate_key[s] * ei
        s_kf[s, :] = k[s] * fo
        s_rf[s, :] = rate_key[s] * fo
        s_e[c:c + 1, :] = jnp.exp(end)

    yield
    zb = jnp.zeros((64, 128), BF)
    zf = jnp.zeros((64, 128), F32)

    def only(x, m):
        return jnp.where(m, x, zb if x.dtype == BF else zf)

    right = jnp.logical_not(left)
    cat = jnp.concatenate
    group = 4
    state = jnp.zeros((128, 128), F32)
    for g in range(chunks // group):
        cs = [slice(64 * c, 64 * c + 64) for c in range(g * group, (g + 1) * group)]
        G0, G1, PW, X, VL, VR = [], [], [], [], [], []
        for s in cs:
            a, qq = s_a[s, :], s_q[s, :]
            ki, ri = s_ki[s, :], s_ri[s, :]
            G0.append(dg3(cat([only(a, left), only(qq, left)], 0), cat([ri, ki], 0), 1, 1))
            G1.append(dg3(cat([only(a, right), only(qq, right)], 0), cat([ki, ri], 0), 1, 1))
        for i, s in enumerate(cs):
            vs = s_vs[s, :]
            VR.append(only(vs, right))
            VL.append(only(vs, left))
            L = cat([only(G0[i][:64], sr), only(G1[i][:64], sl)], 0)
            PW.append(cat([only(G0[i][:64], sl), only(G1[i][:64], sr)], 0))
            a = s_a[s, :]
            X.append(cat([only(a, left), only(a, right)], 0) + dg3(L, cat([VL[i], VR[i]], 0), 1, 0))
        for it in range(6):
            for i in range(group):
                if it < 5:
                    px = dg3(PW[i], cat([PW[i], X[i]], 1), 1, 0)
                    PW[i] = px[:, :128]
                    X[i] = X[i] + px[:, 128:]
                else:
                    X[i] = X[i] + dg3(PW[i], X[i], 1, 0)
        MM, NN, PC, OO = [], [], [], []
        for i, s in enumerate(cs):
            x16 = X[i]
            h0 = cat([x16[:64], VR[i]], 0)
            h1 = cat([VL[i], x16[64:]], 0)
            y0 = dg3(only(G0[i][64:], upto), h0, 1, 0)
            y1 = dg3(only(G1[i][64:], upto), h1, 1, 0)
            qq = s_q[s, :]
            PC.append(cat([only(y0 + qq, left), only(y1 + qq, right)], 0))
            OO.append(only(y0, right) + only(y1, left))
            kf, rf = s_kf[s, :], s_rf[s, :]
            f = cat([only(rf, left), only(kf, left), only(kf, right), only(rf, right)], 0)
            tr = dg3(cat([h0, h1], 0), f, 0, 0)
            e = s_e[g * group + i:g * group + i + 1, :]
            zz = jnp.zeros((128, 128), F32)
            MM.append(jnp.where(same, tr, zz) + jnp.where(eye, e, zz))
            NN.append(jnp.where(same, zz, tr))
        for i, s in enumerate(cs):
            o = dg3(PC[i], state, 1, 1)
            s_o[s, :] = OO[i] + o[:64] + o[64:]
            state = dg3(state, MM[i], 1, 0) + NN[i]
        yield
    o = pltpu.roll(s_o[...], 64, 1)
    centred = o - exact_sum_dot(ones, o, 1, 0, True) * (1.0 / 64)
    spread = exact_sum_dot(ones, centred * centred, 1, 0, True) * (1.0 / 64)
    out[...] = (centred * lax.rsqrt(spread + 0.00064) * gain[...]).astype(BF)


ORDER = (0, 1, 6, 7, 2, 3, 8, 9, 4, 5, 10, 11)


def remote(src, dst, send, recv, **device):
    return pltpu.make_async_remote_copy(
        src_ref=src, dst_ref=dst, send_sem=send, recv_sem=recv, device_id=device,
        device_id_type=MESH)


def meet(peers):
    barrier = pltpu.get_barrier_semaphore()
    for device in peers:
        pl.semaphore_signal(barrier, inc=1, device_id=device, device_id_type=MESH)
    return lambda: pl.semaphore_wait(barrier, len(peers))


def slot_list(ids, z, x):
    row = lax.broadcasted_iota(jnp.int32, (64, 128), 0)
    lane = lax.broadcasted_iota(jnp.int32, (64, 128), 1)
    valid = (row - 8 * (row // 8) < 4) & (lane < 8)
    p = ids.reshape(64, 128).astype(F32)
    plane = jnp.floor((p + 0.5) * (1.0 / 48))
    owner = jnp.floor((p + 0.5) * (1.0 / 12))
    step = owner - 4 * plane - x.astype(F32)
    step = jnp.where(step < 0, step + 4, step)
    slot = step * 12 + p - 12 * owner
    hit = valid & (plane == z.astype(F32))
    m = jnp.where(hit, 1.0, 0.0)
    r1 = lax.broadcasted_iota(jnp.int32, (64, 64), 0)
    c1 = lax.broadcasted_iota(jnp.int32, (64, 64), 1)
    r2 = lax.broadcasted_iota(jnp.int32, (128, 128), 0)
    c2 = lax.broadcasted_iota(jnp.int32, (128, 128), 1)
    near = r1 // 8 == c1 // 8
    above = bdot(jnp.where(near & (c1 < r1), 1.0, 0.0), m)
    column = bdot(jnp.where(near, 1.0, 0.0), m)
    pos = above + bdot(column, jnp.where(r2 < c2, 1.0, 0.0))
    pos = jnp.where(hit, pos, -1.0)
    lanes = lane.astype(F32)
    acc = jnp.zeros((64, 128), F32)
    for b in range(8):
        at = pos[:, b:b + 1]
        acc = acc + jnp.where(at == lanes, slot[:, b:b + 1], 0.0)
        acc = acc + jnp.where((at == lanes - 64) & (at >= 0), b + 1.0, 0.0)
    return jnp.sum(acc.reshape(8, 8, 128), axis=1).astype(jnp.int32)


PIPES = (("st_up", 0, (4, 3, 2, 1)), ("st_down", 1, (4, 5, 6, 7)),
         ("st_up", 1, (3, 2, 1)), ("st_down", 0, (5, 6, 7)))


class Spread:
    def __init__(self, own, buf, send, recv, yp, ym, sib):
        self.copies = []
        for h in range(2):
            s = own.at[pl.ds(256 * h, 256), :]
            links = [(s, buf.at[1, 0, h], sib), (s, buf.at[0, 3, h], yp), (s, buf.at[0, 1, h], ym),
                     (buf.at[0, 3, h], buf.at[1, 3, h], sib), (buf.at[0, 1, h], buf.at[1, 1, h], sib),
                     (buf.at[0, 3, h], buf.at[0, 2, h], yp) if h == 0
                     else (buf.at[0, 1, h], buf.at[0, 2, h], ym),
                     (buf.at[0, 2, h], buf.at[1, 2, h], sib)]
            self.copies.append([
                remote(a, b, send.at[h, k], recv.at[h, k], tp=to) for k, (a, b, to) in enumerate(links)])

    def first(self, h):
        c = self.copies[h]
        for k in ((1, 2, 0) if h == 0 else (2, 1, 0)):
            c[k].start()

    def second(self, h):
        c = self.copies[h]
        if h == 0:
            c[1].wait_recv()
            c[5].start()
            c[3].start()
            c[2].wait_recv()
            c[4].start()
        else:
            c[2].wait_recv()
            c[5].start()
            c[4].start()
            c[1].wait_recv()
            c[3].start()

    def third(self, h):
        self.copies[h][5].wait_recv()
        self.copies[h][6].start()

    def arrived(self, h, *which):
        for k in which:
            self.copies[h][k].wait_recv()


def layer_kernel(store, wk, wv, tok, wq, wg, mq, mk, mv, wc, wm, wgu, qgain, ids, wdl, wdu, base, shift, wrl,
                 wru, gain, out,
                 sv, wkv, wvv, tokv, wqv, wgv, mqv, mkv, mvv, wcv, wmv, wguv, ks, vs0, vs1, qq, idv, lstv, lst,
                 glow, heads, s_a, s_q, s_ki, s_ri, s_kf, s_rf, s_vs, s_e, s_o,
                 kd, vd, pbuf, part, den, msg, box, head_all, att, att_all, gate, mixed,
                 in_sem, k_s, k_r, kh_s, kh_r, v_s, v_r, vh_s, vh_r, zs, zr, ids_s, ids_r, ps, pr, sp_s, sp_r):
    vs = (vs0, vs1)
    st, tp = lax.axis_index("st"), lax.axis_index("tp")
    z, x = st // NX, lax.rem(st, NX)
    y, core = tp // 2, lax.rem(tp, 2)
    xp = z * NX + lax.rem(x + 1, NX)
    xm = z * NX + lax.rem(x + NX - 1, NX)
    zp = lax.rem(z + 1, NZ) * NX + x
    zm = lax.rem(z + NZ - 1, NZ) * NX + x
    yp = lax.rem(y + 1, 4) * 2 + core
    ym = lax.rem(y + 3, 4) * 2 + core
    sib = y * 2 + 1 - core
    ready = meet([{"st": xp}, {"st": xm}, {"st": zp}, {"st": zm}, {"tp": yp}, {"tp": ym}, {"tp": sib}])
    loads = {}

    def load(name, src, dst):
        loads[name] = pltpu.make_async_copy(src, dst, in_sem.at[len(loads)])
        loads[name].start()

    load("tok", tok, tokv)
    load("wq", wq, wqv)
    load("wk", wk, wkv)
    load("wv", wv, wvv)
    for p, i in enumerate(ORDER):
        load(i, store.at[i], sv.at[p])
    for name, src, dst in (("wg", wg, wgv), ("mq", mq, mqv), ("mk", mk, mkv), ("mv", mv, mvv),
                           ("wm", wm, wmv), ("wgu", wgu, wguv), ("wc", wc, wcv)):
        load(name, src, dst)

    def six(ref, at, n=6):
        return ref.at[pl.ds(at, n)]

    left = [remote(six(ks, a, n), six(ks, 12 + a, n), k_s.at[0, i], k_r.at[0, i], st=xm)
            for i, (a, n) in enumerate(((0, 2), (2, 2), (4, 2), (6, 6)))]
    right = [remote(six(ks, a, n), six(ks, 36 + a, n), k_s.at[1, i], k_r.at[1, i], st=xp)
             for i, (a, n) in enumerate(((6, 2), (8, 2), (10, 2), (0, 6)))]

    khop = [remote(six(ks, 12), six(ks, 24), kh_s.at[0], kh_r.at[0], st=xm),
            remote(six(ks, 42), six(ks, 30), kh_s.at[1], kh_r.at[1], st=xp)]
    vleft = [[remote(six(vs[c], 6 * i), six(vs[c], 12 + 6 * i), v_s.at[c, 0, i], v_r.at[c, 0, i], st=xm)
              for i in range(2)] for c in range(2)]
    vright = [[remote(six(vs[c], 6 * i), six(vs[c], 36 + 6 * i), v_s.at[c, 1, i], v_r.at[c, 1, i], st=xp)
               for i in range(2)] for c in range(2)]
    vhop = [[remote(six(vs[c], 12), six(vs[c], 24), vh_s.at[c, 0], vh_r.at[c, 0], st=xm),
             remote(six(vs[c], 42), six(vs[c], 30), vh_s.at[c, 1], vh_r.at[c, 1], st=xp)]
            for c in range(2)]

    def v_start(c):
        vleft[c][0].start()
        vright[c][1].start()
        vleft[c][1].start()
        vright[c][0].start()

    def v_hop(c):
        vleft[c][0].wait_recv()
        vhop[c][0].start()
        vright[c][1].wait_recv()
        vhop[c][1].start()

    def v_wait(c):
        vleft[c][1].wait_recv()
        vright[c][0].wait_recv()
        vhop[c][0].wait_recv()
        vhop[c][1].wait_recv()

    pieces, id_steps = {}, []
    for s in range(4):
        a, b = (8 - s) % 8, 7 - s
        for h in range(2):
            at = pl.ds(256 * h, 256)
            both = []
            if s < 3 or h == 0:
                both.append(remote(qq.at[a, at, :], qq.at[b, at, :], zs.at[0, s, h], zr.at[0, s, h], st=zp))
            if s < 3 or h == 1:
                both.append(remote(qq.at[s, at, :], qq.at[s + 1, at, :], zs.at[1, s, h], zr.at[1, s, h], st=zm))
            pieces[s, h] = both
        steps = [remote(idv.at[a], idv.at[b], ids_s.at[0, s], ids_r.at[0, s], st=zp)]
        if s < 3:
            steps.append(remote(idv.at[s], idv.at[s + 1], ids_s.at[1, s], ids_r.at[1, s], st=zm))
        id_steps.append(steps)

    def z_start(s, h):
        for c in pieces[s, h]:
            c.start()

    def z_wait(s, h):
        for c in pieces[s, h]:
            c.wait_recv()

    def z_pass(s, h):
        z_wait(s, h)
        z_start(s + 1, h)

    def ids_start(s):
        for c in id_steps[s]:
            c.start()

    def ids_wait(s):
        for c in id_steps[s]:
            c.wait_recv()

    idv[0] = jnp.zeros((8, 128), jnp.int32)
    idv[0, 0:4, 0:8] = ids[...]
    loads["tok"].wait()
    loads["wq"].wait()
    proj = dg(tokv[...], wqv[...], 1, 0)
    qq[0] = (head_normed(proj) * qgain[...]).astype(BF) * BF(0.0625)
    ready()
    ids_start(0)
    z_start(0, 0)
    z_start(0, 1)
    loads["wk"].wait()
    loads["wv"].wait()
    for g in range(3):
        for i in ORDER[4 * g:4 * g + 4]:
            loads[i].wait()
        r = sv[4 * g:4 * g + 4].reshape(384, sv.shape[2])
        k = head_normed(dg(r, wkv[...], 1, 0)).astype(BF)
        for u, i in enumerate(ORDER[4 * g:4 * g + 4]):
            ks[i] = k[96 * u:96 * u + 96]
        left[g].start()
        right[g].start()
    left[3].start()
    right[3].start()
    ids_wait(0)
    ids_start(1)
    for g in range(3):
        v = dg(sv[4 * g:4 * g + 4].reshape(384, sv.shape[2]), wvv[...], 1, 0).astype(BF)
        for u, i in enumerate(ORDER[4 * g:4 * g + 4]):
            vs0[i] = v[96 * u:96 * u + 96, 0:128]
            vs1[i] = v[96 * u:96 * u + 96, 128:256]
    ids_wait(1)
    ids_start(2)
    for name in ("wg", "mq", "mk", "mv"):
        loads[name].wait()
    glow[...] = dg(tokv[...], wgv[...], 1, 0).astype(BF)
    stages = mixer_stages(tokv, mqv, mkv, mvv, wdl, wdu, base, shift, wrl, wru, gain, heads,
                          s_a, s_q, s_ki, s_ri, s_kf, s_rf, s_vs, s_e, s_o)
    ids_wait(2)
    ids_start(3)
    z_pass(0, 0)
    next(stages)
    z_pass(0, 1)
    next(stages)
    ids_wait(3)
    lstv[...] = slot_list(idv[...], z, x)
    put = pltpu.make_async_copy(lstv, lst, in_sem.at[len(loads)])
    put.start()
    for i in range(3):
        left[i].wait_recv()
    khop[0].start()
    for i in range(3):
        right[i].wait_recv()
    khop[1].start()
    v_start(0)
    z_pass(1, 0)
    next(stages)
    z_pass(1, 1)
    next(stages)
    z_pass(2, 0)
    for _ in stages:
        pass
    hspread = Spread(heads, head_all, sp_s.at[0], sp_r.at[0], yp, ym, sib)
    hspread.first(0)
    hspread.first(1)
    loads["wgu"].wait()
    loads["wm"].wait()
    loads["wc"].wait()
    gate[...] = jax.nn.sigmoid(dg(glow[...], wguv[...], 1, 0))
    put.wait()
    z_pass(2, 1)

    lane = lax.broadcasted_iota(jnp.int32, (8, 768), 1)
    r128 = lax.broadcasted_iota(jnp.int32, (128, 768), 0)
    diag = lax.broadcasted_iota(jnp.int32, (64, 128), 0) == lax.broadcasted_iota(jnp.int32, (64, 128), 1)

    def slot(d, r):
        return jnp.minimum(jnp.maximum(lst[d, r], 0), 47)

    def scores(d, u):
        block = jnp.zeros((8, 768), jnp.int32)
        for r in range(8):
            kd[u, 96 * r:96 * r + 96, :] = ks[slot(d, r)]
            block = jnp.where((lane >= 96 * r) & (lane < 96 * r + 96), lst[d, 64 + r], block)
        block = block[0:1]
        sums = []
        for t in range(4):
            s = slice(128 * t, 128 * t + 128)
            p = jnp.exp(dg(qq[d, s, :], kd[u], 1, 1))
            p = jnp.where(r128 // 64 + (2 * t + 1) == block, p, 0.0)
            pbuf[d, s, :] = p.astype(BF)
            total = jnp.sum(p, axis=1, keepdims=True)
            for v in range(2):
                line = jnp.where(diag, total[64 * v:64 * v + 64], 0.0)
                sums.append(jnp.sum(line, axis=0, keepdims=True))
        den[8 * d:8 * d + 8, :] = jnp.concatenate(sums, axis=0)

    def values(c, d, u):
        for r in range(8):
            vd[u, 96 * r:96 * r + 96, :] = vs[c][slot(d, r)]
        part[c, d] = dg(pbuf[d], vd[u], 1, 0)

    hspread.second(0)
    hspread.second(1)
    left[3].wait_recv()
    right[3].wait_recv()
    khop[0].wait_recv()
    khop[1].wait_recv()
    v_hop(0)
    v_start(1)
    for n, d in enumerate((0, 1, 7)):
        scores(d, n % 2)
    scores(2, 1)
    scores(6, 0)
    scores(3, 1)
    scores(5, 0)
    origin = [[lax.rem(y + r, 4) * 2 + (core if c == 0 else 1 - core) for r in range(4)] for c in range(2)]
    rest = [(c, r) for c in range(2) for r in range(4) if (c, r) != (0, 0)]

    def weight(w, size, c, r, shift_rows):
        at = pl.multiple_of(origin[c][r] * size + shift_rows, 128)
        return w[pl.ds(at, 128), :]

    hspread.third(0)
    hspread.third(1)
    z_wait(3, 0)
    z_wait(3, 1)
    scores(4, 1)
    for h in range(2):
        hspread.arrived(h, 0, 3, 4, 6)
        m = dg(heads[256 * h:256 * h + 256, :], weight(wmv, 128, 0, 0, 0), 1, 0)
        for c, r in rest:
            m = m + dg(head_all[c, r, h], weight(wmv, 128, c, r, 0), 1, 0)
        mixed[256 * h:256 * h + 256, :] = m

    to = {"st_up": zp, "st_down": zm}

    def box_rows(ref, c, p, s):
        return ref.at[c, p, s] if c == 0 else ref.at[c, p, s, pl.ds(0, 256), :]

    sends = [[[remote(box_rows(msg, c, p, s), box_rows(box, c, p, s), ps.at[c, p, s], pr.at[c, p, s], st=to[way])
               for s in range(len(ds))] for p, (way, _, ds) in enumerate(PIPES)] for c in range(2)]

    def own(c, d, h):
        return part[c, d, 256 * h:256 * h + 256, :], den[8 * d:8 * d + 8, 0:64]

    def held(c, p, s):
        n = box[c, p, s, 0:256, :].astype(F32)
        if c == 1:
            return n, 0.0
        line = box[c, p, s, 256:272, :].astype(F32)[0:8]
        return n, line[:, 0:64] + line[:, 64:128]

    def send(c, p, s):
        _, h, ds = PIPES[p]
        n, d = own(c, ds[s], h)
        if s:
            sends[c][p][s - 1].wait_recv()
            n2, d2 = held(c, p, s - 1)
            n, d = n + n2, d + d2
        msg[c, p, s, 0:256, :] = n.astype(BF)
        if c == 0:
            hi = d.astype(BF).astype(F32)
            line = jnp.concatenate([hi, d - hi], axis=1)
            msg[c, p, s, 256:272, :] = jnp.concatenate([line, jnp.zeros((8, 128), F32)], axis=0).astype(BF)
        sends[c][p][s].start()

    inverse = [None, None]
    spread = [Spread(att.at[c], att_all.at[c], sp_s.at[1 + c], sp_r.at[1 + c], yp, ym, sib) for c in range(2)]

    def settle(c):
        for h, pipes in ((0, (3, 0)), (1, (2, 1))):
            n, d = own(c, 0, h)
            for p in pipes:
                s = len(PIPES[p][2]) - 1
                sends[c][p][s].wait_recv()
                n2, d2 = held(c, p, s)
                n, d = n + n2, d + d2
            if c == 0:
                inverse[h] = jnp.transpose(1.0 / d)
            for b in range(4):
                col = 4 * h + b
                att[c, 256 * h + 64 * b:256 * h + 64 * b + 64, :] = (
                    n[64 * b:64 * b + 64] * inverse[h][:, col:col + 1]).astype(BF)
            spread[c].first(h)

    def begin(c):
        values(c, 4, 0)
        send(c, 0, 0)
        send(c, 1, 0)
        values(c, 3, 1)
        send(c, 2, 0)
        values(c, 5, 0)
        send(c, 3, 0)

    def others(c):
        for n, d in enumerate((2, 6, 1, 7, 0)):
            values(c, d, (n + 1) % 2)

    def step(c, s):
        for p in range(4):
            if s < len(PIPES[p][2]):
                send(c, p, s)

    def add(acc, c, h, which):
        for q, r in which:
            acc = acc + dg(att_all[c, q, r, h], weight(wcv, 256, q, r, 128 * c), 1, 0)
        return acc

    v_wait(0)
    begin(0)
    v_hop(1)
    others(0)
    step(0, 1)
    v_wait(1)
    begin(1)
    step(0, 2)
    others(1)
    step(1, 1)
    step(0, 3)
    step(1, 2)
    settle(0)
    step(1, 3)
    spread[0].second(0)
    spread[0].second(1)
    settle(1)
    spread[0].third(0)
    spread[0].third(1)
    acc = []
    for h in range(2):
        s = slice(256 * h, 256 * h + 256)
        a = dg(att[0, s, :], weight(wcv, 256, 0, 0, 0), 1, 0)
        acc.append(a + dg(att[1, s, :], weight(wcv, 256, 0, 0, 128), 1, 0))
        spread[0].arrived(h, 0, 3, 4)
        acc[h] = add(acc[h], 0, h, rest[:-2] + rest[-1:])
    spread[1].second(0)
    spread[1].second(1)
    for h in range(2):
        spread[0].arrived(h, 6)
        acc[h] = add(acc[h], 0, h, rest[-2:-1])
        spread[1].arrived(h, 0)
        acc[h] = add(acc[h], 1, h, ((0, 3), (0, 1), (1, 0)))
    spread[1].third(0)
    spread[1].third(1)
    for h in range(2):
        spread[1].arrived(h, 3, 4)
        acc[h] = add(acc[h], 1, h, ((0, 2), (1, 1), (1, 3)))
    for h in range(2):
        spread[1].arrived(h, 6)
        c = add(acc[h], 1, h, ((1, 2),))
        s = slice(256 * h, 256 * h + 256)
        out[s, :] = (mixed[s, :] + gate[s, :] * c).astype(BF)
    for group in (left, right, khop, *vleft, *vright, *vhop, *pieces.values(), *id_steps,
                  *sends[0], *sends[1], *(p for sp in (hspread, *spread) for p in sp.copies)):
        for c in group:
            c.wait_send()


def local(
    tokens, mix_query, mix_key, mix_value, decay_lower_map, decay_upper_map, decay_base,
    decay_shift, rate_lower_map, rate_upper_map, norm_gain, mix_out, cross_query, score_gain,
    passage_key, passage_value, cross_out, gate_down, gate_up, store, passage_ids,
):
    rows, width = tokens.shape
    sds = jax.ShapeDtypeStruct
    vm = pltpu.VMEM
    dma = pltpu.SemaphoreType.DMA
    f = lambda: vm((rows, 128), F32)
    b = lambda: vm((rows, 128), BF)
    w256 = lambda: vm((width, 256), BF)
    w128 = lambda: vm((width, 128), BF)
    return pl.pallas_call(
        layer_kernel,
        out_shape=sds((rows, 256), BF),
        in_specs=[ANY] * 12 + [VMEM] * 9,
        out_specs=VMEM,
        scratch_shapes=[
            vm((12, 96, width), BF), w256(), w256(), vm((rows, width), BF), w256(), w128(), w128(),
            w128(), w128(), vm(cross_out.shape, BF), vm(mix_out.shape, BF), vm(gate_up.shape, BF),
            vm((48, 96, 256), BF), vm((48, 96, 128), BF), vm((48, 96, 128), BF), vm((NZ, rows, 256), BF),
            vm((8, 8, 128), jnp.int32), vm((8, 128), jnp.int32), pltpu.SMEM((8, 128), jnp.int32), b(), b(),
            f(), f(), f(), f(), f(), f(), f(), vm((8, 128), F32), f(),
            vm((2, 768, 256), BF), vm((2, 768, 128), BF), vm((NZ, rows, 768), BF),
            vm((2, NZ, rows, 128), F32), vm((64, 128), F32),
            vm((2, 4, 4, 272, 128), BF), vm((2, 4, 4, 272, 128), BF), vm((2, 4, 2, 256, 128), BF),
            vm((2, rows, 128), BF), vm((2, 2, 4, 2, 256, 128), BF), vm((rows, 256), F32), vm((rows, 256), F32),
            dma((24,)), dma((2, 4)), dma((2, 4)), dma((2,)), dma((2,)), dma((2, 2, 2)), dma((2, 2, 2)),
            dma((2, 2)), dma((2, 2)), dma((2, 4, 2)), dma((2, 4, 2)), dma((2, 4)), dma((2, 4)),
            dma((2, 4, 4)), dma((2, 4, 4)), dma((3, 2, 7)), dma((3, 2, 7)),
        ],
        compiler_params=params(62, collective_id=0, has_side_effects=True),
        cost_estimate=cost(3e10),
        name="layer",
    )(store, passage_key, passage_value, tokens, cross_query, gate_down, mix_query, mix_key, mix_value,
      cross_out, mix_out, gate_up, score_gain[None], passage_ids.T, decay_lower_map.T, decay_upper_map,
      decay_base[None], decay_shift.T, rate_lower_map.T, rate_upper_map, norm_gain[None])


def solution(mesh):
    placed = (
        P("st", None), P(None, "tp"), P(None, "tp"), P(None, "tp"), P(), P(None, "tp"), P("tp"),
        P("st", "tp"), P(), P(None, "tp"), P("tp"), P(None, "tp"), P(None, "tp"), P("tp"),
        P(None, "tp"), P(None, "tp"), P(None, "tp"), P(), P(None, "tp"), P("st", None, None),
        P("st", None),
    )
    return jax.shard_map(
        local, mesh=mesh, in_specs=placed, out_specs=P("st", "tp"), check_vma=False)
```
